256 devices in a mesh: grp: 2 (over z), ep: 64 (over y, x), tp: 2 (over core).
Axes of the slice: x: 8, y: 8, z: 2, core: 2. Of those that a mesh axis runs over, the one named last changes fastest.
The devices are a block of a 8x8x16 slice.
Arguments:
- tokens: bfloat16 [4096, 2048], P(('grp', 'ep')), parts along dimension 0, may hold values from -6 to 6
- in_gain: bfloat16 [2048], replicated, may hold values from 0.099609375 to 1.8984375
- route_expert: int32 [4096, 6], P(('grp', 'ep')), parts along dimension 0, may hold values from 0 to 63, all different within a row; in each aligned block of 32 rows (0 to 31, 32 to 63, ...) at most 4 rows name the same one
- route_weight: float32 [4096, 6], P(('grp', 'ep')), parts along dimension 0, may hold values from 0.05 to 1
- gate_weight: bfloat16 [64, 2048, 768], P('ep', None, 'tp'), may hold values from -0.125 to 0.125
- up_weight: bfloat16 [64, 2048, 768], P('ep', None, 'tp'), may hold values from -0.125 to 0.125
- down_weight: bfloat16 [64, 768, 2048], P('ep', 'tp'), may hold values from -1 to 1
- shared_gate: bfloat16 [2048, 768], P(None, 'tp'), may hold values from -0.125 to 0.125
- shared_up: bfloat16 [2048, 768], P(None, 'tp'), may hold values from -0.125 to 0.125
- shared_down: bfloat16 [768, 2048], P('tp'), may hold values from -1 to 1
- out_gain: bfloat16 [2048], P('tp'), may hold values from 0.099609375 to 1.8984375
Outputs:
- mixed: bfloat16 [4096, 2048], P(('grp', 'ep'), 'tp'), parts along dimension 0
The draws below stay inside these ranges and needn't reach their ends.
There are 2 independent parts, one for each index of `grp`. The reference program is written for one: setup_inputs(seed, part) draws one part's arguments, and reference() takes and returns one part's arrays. A program takes and returns all parts, laid end to end along the dimension named above; an argument that names none is the same for every part. Nothing has to cross between parts.
Inputs may be any that keep to these rules, and one draw needn't show every extreme that they name: `route_expert`: each row names 6 different experts. Among the rows of one device no expert is named more than 4 times, a bound that some block reaches.
All inputs are finite; a program needn't handle non-finite values.
Results may differ from the reference program's by a relative error of at most 0.0077.
Values may be sent and summed in bfloat16 or wider, within the bound.
A program may use at most 64 MiB of HBM per device.

```python
import math
import jax
import jax.numpy as jnp
import numpy as np
from jax import lax

D = 2048
FE = 768
FS = 768
TOPK = 6
TOK_DEV = 32
EXPERTS = 64
CAP = 4
TOKENS = 2048
N_EP = 64
N_TP = 2


def down_matrix(key, fan_in, copies, columns):
    position = jnp.arange(columns, dtype=jnp.float32) / columns
    draws = jnp.clip(jax.random.normal(key, (copies, fan_in, columns), jnp.float32), -4.0, 4.0)
    factor = 0.5 * 3.0 ** position
    return draws * factor[None, None, :] * fan_in ** (-0.5)


def draw_down_weight(key, part):
    return down_matrix(jax.random.fold_in(key, 11), FE, EXPERTS, D).astype(jnp.bfloat16)


def draw_shared_down(key, part):
    return down_matrix(jax.random.fold_in(key, 23), FS, 1, D)[0].astype(jnp.bfloat16)


def block_scale(own_key, extent, cuts, low, top_value):
    loudness, own = 1.0, jax.random.fold_in(own_key, 6)
    for dim, shards_of in cuts:
        heights = jnp.exp(jax.random.uniform(jax.random.fold_in(own, dim), (shards_of,), jnp.float32, low / len(cuts), top_value / len(cuts)))
        loudness = loudness * jnp.repeat(heights, extent[dim] // shards_of).reshape([-1 if axis == dim else 1 for axis in range(len(extent))])
    return loudness


def shared_out(rng, own, number, rows, number_of, top, reach, skew):
    ranking = jax.random.permutation(rng, number_of)
    crowded, ordinary = portions_of(number_of, rows * top, reach, skew, True), portions_of(number_of, rows * top, reach, skew, False)
    places = jnp.arange(number_of)

    def named(lengths, offset_by):
        used = int((lengths > 0).sum())
        fixed = max(1, used // 4)
        moved = fixed + (places - fixed + offset_by * (used - fixed)) % max(1, number_of - fixed)
        return jnp.zeros((number_of,), jnp.int32).at[ranking[jnp.where(places < fixed, places, moved)]].set(jnp.asarray(lengths, jnp.int32))

    lengths = jnp.where(number % 4 == 0, named(crowded, number // 4), named(ordinary, number - number // 4 - 1))
    mixed = jax.random.permutation(jax.random.fold_in(own, 3), number_of)
    giver, receiver = mixed[0:number_of // 2 * 2:2], mixed[1:number_of // 2 * 2:2]
    slack = jnp.minimum(lengths[giver] - 1, reach - lengths[receiver]) // 2
    slack = jnp.where((giver == ranking[0]) | (receiver == ranking[0]) | (lengths[receiver] == 0), 0, jnp.maximum(slack, 0))
    moved = jax.random.randint(jax.random.fold_in(own, 4), (number_of // 2,), 0, 1 << 20) % (slack + 1)
    lengths = lengths.at[giver].add(-moved).at[receiver].add(moved)
    members = jnp.searchsorted(jnp.cumsum(lengths), jnp.arange(rows * top), side="right").astype(jnp.int32)
    grid = members.reshape(top, rows).T
    grid = grid[jax.random.permutation(jax.random.fold_in(own, 1), rows)]
    offset_by = jax.random.randint(jax.random.fold_in(own, 2), (rows, 1), 0, top)
    return jnp.take_along_axis(grid, (jnp.arange(top)[None, :] + offset_by) % top, axis=1)


def portions_of(amount, total, reach, lean, full):
    weights = [(1 << 20) // math.isqrt(grade ** lean) + 1 for grade in range(1, amount + 1)]
    largest = reach if full else min(reach, max(-(-total // amount), total * weights[0] // sum(weights)))
    least = 1 if total - largest >= amount - 1 else 0
    holding, rest = [largest] + [least] * (amount - 1), total - largest - least * (amount - 1)
    while rest > 0:
        free = [i for i in range(1, amount) if holding[i] < largest] or [i for i in range(1, amount) if holding[i] < reach]
        pool, left = sum([weights[i] for i in free]), rest
        for i in free:
            extra = min(reach - holding[i], max(1, left * weights[i] // pool), rest)
            holding[i] = holding[i] + extra
            rest = rest - extra
    return np.array(holding)


def scatter_about(key, shape, spread, reach, shards=(), kind=jnp.bfloat16):
    loudness = block_scale(key, shape, shards, -0.22, 0.18) if shards else 1.0
    array = jax.random.normal(key, shape, jnp.float32) * spread * loudness
    return jnp.minimum(jnp.maximum(array, -reach), reach).astype(kind)


def setup_inputs(seed: int = 0, part: int = 0) -> dict:
    keys = jax.random.split(jax.random.key(seed), 12)
    own_keys = jax.random.split(jax.random.fold_in(keys[11], part), 12)
    tokens = scatter_about(own_keys[0], (TOKENS, D), 1.0, 6.0, ((0, 64),))
    in_gain = jnp.clip(1.0 + 0.18 * jax.random.normal(keys[1], (D,), jnp.float32), 0.099609375, 1.8984375).astype(jnp.bfloat16)
    route_expert_keys = jax.random.split(jax.random.fold_in(own_keys[2], 1), TOKENS // TOK_DEV)
    route_expert_turns = jax.random.permutation(jax.random.fold_in(own_keys[2], 3), TOKENS // TOK_DEV)
    route_expert = jax.vmap(lambda own, number: shared_out(jax.random.fold_in(own_keys[2], 2), own, number, TOK_DEV, EXPERTS, TOPK, CAP, 2))(route_expert_keys, route_expert_turns).reshape((TOKENS, TOPK))
    route_weight = jnp.clip(jnp.exp(math.log(1.0) - 2.9957323 * jax.random.uniform(own_keys[3], (TOKENS, TOPK), jnp.float32) ** block_scale(own_keys[3], (TOKENS, TOPK), ((0, 64),), -0.2, 0.2)), 0.05, 1.0)
    gate_weight = scatter_about(keys[4], (EXPERTS, D, FE), D ** -0.5, 0.125, ((0, 64), (2, 2)))
    up_weight = scatter_about(keys[5], (EXPERTS, D, FE), D ** -0.5, 0.125, ((0, 64), (2, 2)))
    down_weight = draw_down_weight(jax.random.fold_in(keys[11], 71), part)
    shared_gate = scatter_about(keys[7], (D, FS), D ** -0.5, 0.125, ((1, 2),))
    shared_up = scatter_about(keys[8], (D, FS), D ** -0.5, 0.125, ((1, 2),))
    shared_down = draw_shared_down(jax.random.fold_in(keys[11], 71), part)
    out_gain = jnp.clip(1.0 + 0.18 * jax.random.normal(keys[10], (D,), jnp.float32), 0.099609375, 1.8984375).astype(jnp.bfloat16)
    return dict(tokens=tokens, in_gain=in_gain, route_expert=route_expert, route_weight=route_weight, gate_weight=gate_weight, up_weight=up_weight, down_weight=down_weight, shared_gate=shared_gate, shared_up=shared_up, shared_down=shared_down, out_gain=out_gain)


EPSILON = 1e-06

def normalize(values, gain_vector):
    floats = values.astype(jnp.float32)
    scaled = floats * lax.rsqrt(lax.optimization_barrier(jnp.mean(floats * floats, axis=-1, keepdims=True)) + EPSILON)
    return (scaled * gain_vector.astype(jnp.float32)).astype(jnp.bfloat16)

def swiglu_hidden(inputs, gate_here, up_here):
    gate_value = jnp.dot(inputs, gate_here, preferred_element_type=jnp.float32)
    upward = jnp.dot(inputs, up_here, preferred_element_type=jnp.float32)
    return (jax.nn.silu(gate_value) * upward).astype(jnp.bfloat16)

def split_product(hidden, down_here, pieces):
    inner_width = hidden.shape[1] // pieces
    running = jnp.zeros((hidden.shape[0], down_here.shape[1]), jnp.float32)
    for portion in range(pieces):
        partial_value = jnp.dot(hidden[:, portion * inner_width:(portion + 1) * inner_width], down_here[portion * inner_width:(portion + 1) * inner_width], preferred_element_type=jnp.float32)
        running = running + lax.optimization_barrier(partial_value.astype(jnp.bfloat16)).astype(jnp.float32)
    return running.astype(jnp.bfloat16)

def slot_tables(routes_here, experts, capacity):
    picked_count = routes_here.shape[0] * routes_here.shape[1]
    flattened = routes_here.reshape(picked_count).astype(jnp.int32)
    onehot = (flattened[:, None] == jnp.arange(experts, dtype=jnp.int32)[None, :]).astype(jnp.int32)
    earlier = (jnp.cumsum(onehot, axis=0) - onehot).astype(jnp.int32)
    ranked = lax.optimization_barrier(jnp.sum(earlier * onehot, axis=1)).astype(jnp.int32)
    slot_index = flattened * capacity + ranked
    source_token = jnp.arange(picked_count, dtype=jnp.int32) // routes_here.shape[1]
    matches = slot_index[None, :] == jnp.arange(experts * capacity, dtype=jnp.int32)[:, None]
    filled = jnp.any(matches, axis=1)
    slot_owner = lax.optimization_barrier(jnp.sum(jnp.where(matches, source_token[None, :], 0), axis=1)).astype(jnp.int32)
    return (slot_index, filled, slot_owner)

def reference(tokens, in_gain, route_expert, route_weight, gate_weight, up_weight, down_weight, shared_gate, shared_up, shared_down, out_gain):
    capacity = CAP
    normed = normalize(tokens, in_gain)
    grouped = route_expert.reshape(N_EP, TOK_DEV, TOPK)
    slot_index, filled, slot_owner = jax.vmap(lambda routes_here: slot_tables(routes_here, EXPERTS, capacity))(grouped)
    per_device = normed.reshape(N_EP, TOK_DEV, D)
    outgoing = jax.vmap(lambda rows_here, chosen, filled_here: jnp.where(filled_here[:, None], rows_here[chosen], jnp.zeros((), jnp.bfloat16)))(per_device, slot_owner, filled)
    by_expert = outgoing.reshape(N_EP, EXPERTS, capacity, D).transpose(1, 0, 2, 3).reshape(EXPERTS, N_EP * capacity, D)

    def expert_pass(inputs):
        expert_rows, gate_here, up_here, down_here = inputs
        return split_product(swiglu_hidden(expert_rows, gate_here, up_here), down_here, N_TP)
    results = lax.map(expert_pass, (by_expert, gate_weight, up_weight, down_weight))
    returned = results.reshape(EXPERTS, N_EP, capacity, D).transpose(1, 0, 2, 3).reshape(N_EP, EXPERTS * capacity, D)
    picked = jax.vmap(lambda result_rows, chosen: result_rows[chosen])(returned, slot_index).astype(jnp.float32)
    picked = picked * route_weight.reshape(N_EP, TOK_DEV * TOPK)[:, :, None]
    routed = lax.optimization_barrier(jnp.sum(picked.reshape(TOKENS, TOPK, D), axis=1))
    shared = split_product(swiglu_hidden(normed, shared_gate, shared_up), shared_down, N_TP).astype(jnp.float32)
    combined = shared + routed
    scaled = combined * lax.rsqrt(lax.optimization_barrier(jnp.mean(combined * combined, axis=1, keepdims=True)) + EPSILON)
    return (scaled * out_gain.astype(jnp.float32)).astype(jnp.bfloat16)
```

```python
import functools
import math

import jax
import jax.numpy as jnp
from jax import lax
from jax.experimental import pallas as pl
from jax.experimental.pallas import tpu as pltpu
from jax.sharding import PartitionSpec as P

EPSILON = 1e-06
BF16 = jnp.bfloat16
F32 = jnp.float32
LANES = 128
MESH = pl.DeviceIdType.MESH


def far_first(side):
    def reach(step):
        return min(step, side - step)

    offsets = [(dx, dy) for dy in range(side) for dx in range(side) if dx or dy]
    return sorted(offsets, key=lambda o: -(reach(o[0]) + reach(o[1])))


def dot(a, b):
    return jnp.dot(a, b, preferred_element_type=F32)


def iota(shape, dim):
    return lax.broadcasted_iota(jnp.int32, shape, dim)


def one_hot_to_rows(blocks, per_row):
    size = blocks * per_row
    row, col = iota((size, size), 0), iota((size, size), 1)
    return (col == (row % blocks) * per_row + row // blocks).astype(F32).astype(BF16)


def one_hot_to_blocks(blocks, per_row):
    size = blocks * per_row
    row, col = iota((size, size), 0), iota((size, size), 1)
    return (col == (row % per_row) * blocks + row // per_row).astype(F32).astype(BF16)


def kernel(
    experts, cores, slots,
    tokens_hbm, in_gain_hbm, route_hbm, weight_hbm, gate_hbm, up_hbm, down_hbm, sgate_hbm, sup_hbm, sdown_hbm, out_gain_hbm,
    out_ref,
    tokens, in_gain, route, weight, out_gain, gate, up, down, sgate, sup, sdown,
    normed, tx, rx, rows, tx2, rx2, picks, shared_send, shared_recv, shared_half, sq_send, sq_recv,
    small_sem, weight_sem, push_send, push_recv, send_sem, recv_sem, send2_sem, recv2_sem, pair_send, pair_recv, ready_sem,
):
    ep, c = lax.axis_index("ep"), lax.axis_index("tp")
    other = 1 - c
    side = math.isqrt(experts)
    here_x, here_y = lax.rem(ep, side), lax.div(ep, side)
    local_tokens, width = tokens.shape
    half = width // cores
    chunks = slots // cores
    wide = width // LANES
    thin = half // LANES
    order = far_first(side)

    def peer(offset):
        return lax.rem(here_y + offset[1], side) * side + lax.rem(here_x + offset[0], side)

    small = [
        pltpu.make_async_copy(src, dst, small_sem.at[i])
        for i, (src, dst) in enumerate(
            [(route_hbm, route), (tokens_hbm, tokens), (in_gain_hbm, in_gain), (weight_hbm, weight), (out_gain_hbm, out_gain)]
        )
    ]
    for copy in small:
        copy.start()
    barrier = pltpu.get_barrier_semaphore()
    for offset in order:
        pl.semaphore_signal(barrier, inc=1, device_id={"ep": peer(offset)}, device_id_type=MESH)
    pl.semaphore_signal(barrier, inc=1, device_id={"tp": other}, device_id_type=MESH)
    loads = [
        pltpu.make_async_copy(src, dst, weight_sem.at[i])
        for i, (src, dst) in enumerate(
            [
                (sgate_hbm, sgate), (sup_hbm, sup), (sdown_hbm, sdown),
                (gate_hbm.at[0], gate.at[0]), (up_hbm.at[0], up.at[0]), (down_hbm.at[0], down.at[0]),
            ]
        )
    ]
    for copy in loads:
        copy.start()

    small[0].wait()
    names = route[...]
    expert_lane = iota((local_tokens, LANES), 1)
    hits = [names[:, k : k + 1] == expert_lane for k in range(names.shape[1])]
    chosen = functools.reduce(jnp.logical_or, hits)
    chosen_f = chosen.astype(F32)
    lower = (iota((local_tokens, local_tokens), 0) > iota((local_tokens, local_tokens), 1)).astype(F32).astype(BF16)
    rank = jnp.where(chosen, dot(lower, chosen_f.astype(BF16)), -1.0)
    rank_b = rank.astype(BF16)
    eye = (iota((experts, LANES), 0) == iota((experts, LANES), 1)).astype(F32).astype(BF16)
    rank_t = lax.dot_general(eye, rank_b, (((1,), (1,)), ((), ())), preferred_element_type=F32)

    small[1].wait()
    small[2].wait()
    floats = tokens[...].astype(F32)
    scale = lax.rsqrt(jnp.mean(floats * floats, axis=1, keepdims=True) + EPSILON)
    normed[...] = (floats * scale * in_gain[...].astype(F32)).astype(BF16)

    to_blocks = one_hot_to_blocks(wide, wide)
    per_block = wide
    first_slot = (c * chunks).astype(F32)
    for j in range(chunks):
        pick = (rank_t == first_slot + j).astype(F32).astype(BF16)
        picked = dot(pick, normed[...]).astype(BF16)
        for b in range(experts // per_block):
            part = picked[b * per_block : (b + 1) * per_block]
            stacked = jnp.concatenate([part[:, q * LANES : (q + 1) * LANES] for q in range(wide)], axis=0)
            tx[j, pl.ds(b * per_block, per_block)] = (
                dot(to_blocks, stacked).astype(BF16).reshape(per_block, wide, LANES)
            )
        rx[j, ep] = tx[j, ep]

    pl.semaphore_wait(barrier, experts)
    pl.semaphore_signal(ready_sem, inc=1, device_id={"tp": other}, device_id_type=MESH)

    def dispatch(j, offset):
        to = peer(offset)
        return pltpu.make_async_remote_copy(
            src_ref=tx.at[j, to], dst_ref=rx.at[j, ep], send_sem=send_sem.at[j], recv_sem=recv_sem.at[j],
            device_id={"ep": to}, device_id_type=MESH,
        )

    for j in range(chunks):
        for offset in order:
            dispatch(j, offset).start()
    pushes = [
        pltpu.make_async_remote_copy(
            src_ref=src.at[0], dst_ref=dst.at[1], send_sem=push_send.at[i], recv_sem=push_recv.at[i],
            device_id={"tp": other}, device_id_type=MESH,
        )
        for i, (src, dst) in enumerate([(gate_hbm, gate), (up_hbm, up), (down_hbm, down)])
    ]
    for copy in pushes:
        copy.start()

    def swiglu(inputs, pairs):
        hidden = []
        for gate_here, up_here in pairs:
            gate_value = dot(inputs, gate_here)
            upward = dot(inputs, up_here)
            hidden.append((jax.nn.silu(gate_value) * upward).astype(BF16))
        return hidden

    for copy in loads[:3]:
        copy.wait()
    (hidden,) = swiglu(normed[...], [(sgate[...], sup[...])])
    shared_part = dot(hidden, sdown[...]).astype(BF16)
    for side_of in range(cores):
        shared_send[side_of] = shared_part[:, side_of * half : (side_of + 1) * half]
    pair = pltpu.make_async_remote_copy(
        src_ref=shared_send.at[other], dst_ref=shared_recv, send_sem=pair_send.at[0], recv_sem=pair_recv.at[0],
        device_id={"tp": other}, device_id_type=MESH,
    )
    pair.start()

    small[3].wait()
    small[4].wait()
    weights = weight[...]
    weight_at = functools.reduce(
        jnp.add, [jnp.where(hit, weights[:, k : k + 1], 0.0) for k, hit in enumerate(hits)]
    )
    high = weight_at.astype(BF16)
    low = (weight_at - high.astype(F32)).astype(BF16)
    columns = experts * cores * thin
    col = iota((LANES, columns), 1)
    expand = (iota((LANES, columns), 0) == col // (cores * thin)).astype(F32).astype(BF16)
    spread = dot(jnp.concatenate([high, low, rank_b], axis=0), expand)
    col = iota((local_tokens, columns), 1)
    slot_base = ((col // thin) % cores * chunks).astype(F32)
    q_col = col % thin
    for j in range(chunks):
        here = spread[2 * local_tokens :] == slot_base + j
        for part in range(2):
            value = jnp.where(here, spread[part * local_tokens : (part + 1) * local_tokens], 0.0)
            for q in range(thin):
                picks[j, pl.ds((part * thin + q) * local_tokens, local_tokens)] = jnp.where(
                    q_col == q, value, 0.0
                ).astype(BF16)

    pair.wait()
    for q in range(thin):
        lanes = slice(q * LANES, (q + 1) * LANES)
        total = shared_send[c][:, lanes].astype(F32) + shared_recv[:, lanes].astype(F32)
        shared_half[pl.ds(q * local_tokens, local_tokens)] = total.astype(BF16).astype(F32)

    for copy in loads[3:]:
        copy.wait()
    for copy in pushes:
        copy.wait()
    pl.semaphore_wait(ready_sem, 1)

    to_rows = one_hot_to_rows(wide, wide)
    per_back = 2 * LANES // thin
    to_thin = one_hot_to_blocks(per_back, thin)

    def give_back(j, offset, core):
        to = peer(offset)
        return pltpu.make_async_remote_copy(
            src_ref=tx2.at[j, core, to], dst_ref=rx2.at[j, ep * cores + c], send_sem=send2_sem.at[j], recv_sem=recv2_sem.at[j],
            device_id={"ep": to, "tp": core}, device_id_type=MESH,
        )

    partner_back = []
    for j in range(chunks):
        arrived = rx.at[j, pl.ds(0, experts - 1)]
        pltpu.make_async_copy(arrived, arrived, recv_sem.at[j]).wait()
        for b in range(experts // per_block):
            block = rx[j, pl.ds(b * per_block, per_block)].reshape(per_block * wide, LANES)
            sorted_rows = dot(to_rows, block).astype(BF16)
            for q in range(wide):
                rows[pl.ds(b * per_block, per_block), q * LANES : (q + 1) * LANES] = sorted_rows[
                    q * per_block : (q + 1) * per_block
                ]
        hidden = swiglu(rows[...], [(gate[h], up[h]) for h in range(cores)])
        result = functools.reduce(jnp.add, [dot(hidden[h], down[h]) for h in range(cores)]).astype(BF16)
        for b in range(experts // per_back):
            part = result[b * per_back : (b + 1) * per_back]
            for core in range(cores):
                stacked = jnp.concatenate(
                    [part[:, core * half + q * LANES : core * half + (q + 1) * LANES] for q in range(thin)], axis=0
                )
                tx2[j, core, pl.ds(b * per_back, per_back)] = (
                    dot(to_thin, stacked).astype(BF16).reshape(per_back, thin, LANES)
                )
        for offset in order:
            for core in range(cores):
                give_back(j, offset, core).start()
        back = pltpu.make_async_remote_copy(
            src_ref=tx2.at[j, other, ep], dst_ref=rx2.at[j, ep * cores + c], send_sem=send2_sem.at[j], recv_sem=recv2_sem.at[j],
            device_id={"tp": other}, device_id_type=MESH,
        )
        back.start()
        rx2[j, ep * cores + c] = tx2[j, c, ep]

    total = shared_half[...]
    for j in range(chunks):
        arrived = rx2.at[j, pl.ds(0, experts * cores - 1)]
        pltpu.make_async_copy(arrived, arrived, recv2_sem.at[j]).wait()
        summed = dot(picks[j], rx2[j].reshape(experts * cores * thin, LANES))
        total = total + summed[: thin * local_tokens] + summed[thin * local_tokens :]
    squares = total * total
    mine = functools.reduce(jnp.add, [squares[q * local_tokens : (q + 1) * local_tokens] for q in range(thin)])
    mine = jnp.broadcast_to(jnp.sum(mine, axis=1, keepdims=True), (local_tokens, LANES))
    sq_send[...] = mine
    pair = pltpu.make_async_remote_copy(
        src_ref=sq_send, dst_ref=sq_recv, send_sem=pair_send.at[1], recv_sem=pair_recv.at[1],
        device_id={"tp": other}, device_id_type=MESH,
    )
    pair.start()
    for j in range(chunks):
        sent = tx.at[j, pl.ds(0, experts - 1)]
        pltpu.make_async_copy(sent, sent, send_sem.at[j]).wait()
        sent = rx2.at[j, pl.ds(0, experts * cores - 1)]
        pltpu.make_async_copy(sent, sent, send2_sem.at[j]).wait()
    pair.wait()
    scale = lax.rsqrt((mine + sq_recv[...]) / width + EPSILON)
    gain = out_gain[...].astype(F32)
    for q in range(thin):
        lanes = slice(q * LANES, (q + 1) * LANES)
        out_ref[:, lanes] = (total[q * local_tokens : (q + 1) * local_tokens] * scale * gain[:, lanes]).astype(BF16)


def body(tokens, in_gain, route_expert, route_weight, gate_weight, up_weight, down_weight, shared_gate, shared_up, shared_down, out_gain):
    experts, cores = lax.axis_size("ep"), lax.axis_size("tp")
    local_tokens, width = tokens.shape
    top_count = route_expert.shape[1]
    slots = max(2, (local_tokens * top_count * 4 + 3 * experts - 1) // (3 * experts))
    chunks = slots // cores
    half = width // cores
    wide, thin = width // LANES, half // LANES
    hidden = gate_weight.shape[2]
    any_spec = pl.BlockSpec(memory_space=pl.ANY)
    vmem, dma = pltpu.VMEM, pltpu.SemaphoreType.DMA
    scratch = [
        vmem((local_tokens, width), BF16), vmem((1, width), BF16), vmem((local_tokens, top_count), jnp.int32),
        vmem((local_tokens, top_count), F32), vmem((1, half), BF16),
        vmem((cores, width, hidden), BF16), vmem((cores, width, hidden), BF16), vmem((cores, hidden, width), BF16),
        vmem((width, hidden), BF16), vmem((width, hidden), BF16), vmem((hidden, width), BF16),
        vmem((local_tokens, width), BF16),
        vmem((chunks, experts, wide, LANES), BF16), vmem((chunks, experts, wide, LANES), BF16),
        vmem((experts, width), BF16),
        vmem((chunks, cores, experts, thin, LANES), BF16), vmem((chunks, experts * cores, thin, LANES), BF16),
        vmem((chunks, 2 * thin * local_tokens, experts * cores * thin), BF16),
        vmem((cores, local_tokens, half), BF16), vmem((local_tokens, half), BF16), vmem((thin * local_tokens, LANES), F32),
        vmem((local_tokens, LANES), F32), vmem((local_tokens, LANES), F32),
        dma((5,)), dma((6,)), dma((3,)), dma((3,)), dma((chunks,)), dma((chunks,)), dma((chunks,)), dma((chunks,)),
        dma((2,)), dma((2,)), pltpu.SemaphoreType.REGULAR,
    ]
    return pl.pallas_call(
        functools.partial(kernel, experts, cores, slots),
        out_shape=jax.ShapeDtypeStruct((local_tokens, half), BF16),
        in_specs=[any_spec] * 11,
        out_specs=pl.BlockSpec(memory_space=pltpu.VMEM),
        scratch_shapes=scratch,
        compiler_params=pltpu.CompilerParams(collective_id=0, has_side_effects=True, vmem_limit_bytes=60 * 1024 * 1024),
    )(
        tokens, in_gain.reshape(1, width), route_expert, route_weight, gate_weight, up_weight, down_weight,
        shared_gate, shared_up, shared_down, out_gain.reshape(1, half),
    )


def solution(mesh):
    return jax.shard_map(
        body,
        mesh=mesh,
        in_specs=(
            P(("grp", "ep"), None),
            P(),
            P(("grp", "ep"), None),
            P(("grp", "ep"), None),
            P("ep", None, "tp"),
            P("ep", None, "tp"),
            P("ep", "tp", None),
            P(None, "tp"),
            P(None, "tp"),
            P("tp", None),
            P("tp"),
        ),
        out_specs=P(("grp", "ep"), "tp"),
        check_vma=False,
    )
```

```python
import functools
import math

import jax
import jax.numpy as jnp
from jax import lax
from jax.experimental import pallas as pl
from jax.experimental.pallas import tpu as pltpu
from jax.sharding import PartitionSpec as P

EPSILON = 1e-06
BF16 = jnp.bfloat16
F32 = jnp.float32
LANES = 128
MESH = pl.DeviceIdType.MESH


def far_first(side):
    def reach(step):
        return min(step, side - step)

    offsets = [(dx, dy) for dy in range(side) for dx in range(side) if dx or dy]
    offsets = sorted(offsets, key=lambda o: -(reach(o[0]) + reach(o[1])))
    straight = [o for o in offsets if not (o[0] and o[1])]
    return straight, [o for o in offsets if o[0] and o[1]]


def dot(a, b):
    return jnp.dot(a, b, preferred_element_type=F32)


def iota(shape, dim):
    return lax.broadcasted_iota(jnp.int32, shape, dim)


def one_hot_to_rows(blocks, per_row):
    size = blocks * per_row
    row, col = iota((size, size), 0), iota((size, size), 1)
    return (col == (row % blocks) * per_row + row // blocks).astype(F32).astype(BF16)


def one_hot_to_blocks(blocks, per_row):
    size = blocks * per_row
    row, col = iota((size, size), 0), iota((size, size), 1)
    return (col == (row % per_row) * blocks + row // per_row).astype(F32).astype(BF16)


def kernel(
    experts, cores, slots,
    tokens_hbm, in_gain_hbm, route_hbm, weight_hbm, gate_hbm, up_hbm, down_hbm, sgate_hbm, sup_hbm, sdown_hbm, out_gain_hbm,
    out_ref,
    tokens, in_gain, route, weight, out_gain, gate, up, down, sgate, sup, sdown,
    normed, tx, rx, rows, tx2, rx2, picks, shared_send, shared_recv, shared_half, sq_send, sq_recv,
    small_sem, weight_sem, push_send, push_recv, send_sem, recv_sem, send2_sem, recv2_sem, pair_send, pair_recv, pair_sem, lines_sem, planes_sem,
):
    ep, c = lax.axis_index("ep"), lax.axis_index("tp")
    other = 1 - c
    side = math.isqrt(experts)
    here_x, here_y = lax.rem(ep, side), lax.div(ep, side)
    local_tokens, width = tokens.shape
    half = width // cores
    chunks = slots // cores
    wide = width // LANES
    thin = half // LANES
    straight, diagonal = far_first(side)
    order = diagonal + straight

    def peer(offset):
        return lax.rem(here_y + offset[1], side) * side + lax.rem(here_x + offset[0], side)

    small = [
        pltpu.make_async_copy(src, dst, small_sem.at[i])
        for i, (src, dst) in enumerate(
            [(route_hbm, route), (tokens_hbm, tokens), (in_gain_hbm, in_gain), (weight_hbm, weight), (out_gain_hbm, out_gain)]
        )
    ]
    for copy in small:
        copy.start()
    barrier = pltpu.get_barrier_semaphore()

    @pl.when(c == 0)
    def _():
        pl.semaphore_signal(barrier, inc=1, device_id={"tp": 1}, device_id_type=MESH)

    @pl.when(c == 1)
    def _():
        pl.semaphore_wait(barrier, 1)
        pl.semaphore_signal(pair_sem, inc=1, device_id={"tp": 0}, device_id_type=MESH)

    @pl.when(c == 0)
    def _():
        pl.semaphore_wait(pair_sem, 1)
        for offset in straight:
            pl.semaphore_signal(barrier, inc=1, device_id={"ep": peer(offset)}, device_id_type=MESH)

    pushes = [
        pltpu.make_async_remote_copy(
            src_ref=src.at[0], dst_ref=dst.at[1], send_sem=push_send.at[i], recv_sem=push_recv.at[i],
            device_id={"tp": other}, device_id_type=MESH,
        )
        for i, (src, dst) in enumerate([(gate_hbm, gate), (up_hbm, up), (down_hbm, down)])
    ]
    for copy in pushes:
        copy.start()
    loads = [
        pltpu.make_async_copy(src, dst, weight_sem.at[i])
        for i, (src, dst) in enumerate(
            [
                (sgate_hbm, sgate), (sup_hbm, sup), (sdown_hbm, sdown),
                (gate_hbm.at[0], gate.at[0]), (up_hbm.at[0], up.at[0]), (down_hbm.at[0], down.at[0]),
            ]
        )
    ]
    for copy in loads:
        copy.start()

    small[0].wait()
    names = route[...]
    expert_row = iota((experts, local_tokens), 0)
    hits = [names[k : k + 1, :] == expert_row for k in range(names.shape[0])]
    chosen = functools.reduce(jnp.logical_or, hits)
    earlier = (iota((local_tokens, local_tokens), 0) < iota((local_tokens, local_tokens), 1)).astype(F32).astype(BF16)
    rank_t = jnp.where(chosen, dot(chosen.astype(F32).astype(BF16), earlier), -1.0)

    small[1].wait()
    small[2].wait()
    floats = tokens[...].astype(F32)
    scale = lax.rsqrt(jnp.mean(floats * floats, axis=1, keepdims=True) + EPSILON)
    gains = in_gain[...].astype(F32)
    for q in range(wide):
        lanes = slice(q * LANES, (q + 1) * LANES)
        normed[:, lanes] = (floats[:, lanes] * scale * gains[q : q + 1, :]).astype(BF16)

    to_blocks = one_hot_to_blocks(wide, wide)
    per_block = wide
    first_slot = (c * chunks).astype(F32)
    for j in range(chunks):
        pick = (rank_t == first_slot + j).astype(F32).astype(BF16)
        picked = dot(pick, normed[...]).astype(BF16)
        for b in range(experts // per_block):
            part = picked[b * per_block : (b + 1) * per_block]
            stacked = jnp.concatenate([part[:, q * LANES : (q + 1) * LANES] for q in range(wide)], axis=0)
            tx[j, pl.ds(b * per_block, per_block)] = (
                dot(to_blocks, stacked).astype(BF16).reshape(per_block, wide, LANES)
            )
        rx[j, ep] = tx[j, ep]

    def dispatch(j, offset):
        to = peer(offset)
        return pltpu.make_async_remote_copy(
            src_ref=tx.at[j, to], dst_ref=rx.at[j, ep], send_sem=send_sem.at[j], recv_sem=recv_sem.at[j],
            device_id={"ep": to}, device_id_type=MESH,
        )

    @pl.when(c == 0)
    def _():
        pl.semaphore_wait(barrier, len(straight))
        pl.semaphore_signal(lines_sem, inc=1, device_id={"tp": 1}, device_id_type=MESH)
        for offset in straight:
            if offset[1]:
                pl.semaphore_signal(planes_sem, inc=1, device_id={"ep": peer(offset)}, device_id_type=MESH)

    @pl.when(c == 1)
    def _():
        pl.semaphore_wait(lines_sem, 1)

    for j in range(chunks):
        for offset in straight:
            dispatch(j, offset).start()

    @pl.when(c == 0)
    def _():
        pl.semaphore_wait(planes_sem, side - 1)
        pl.semaphore_signal(lines_sem, inc=1, device_id={"tp": 1}, device_id_type=MESH)

    @pl.when(c == 1)
    def _():
        pl.semaphore_wait(lines_sem, 1)

    for j in range(chunks):
        for offset in diagonal:
            dispatch(j, offset).start()

    def swiglu(inputs, pairs):
        hidden = []
        for gate_here, up_here in pairs:
            gate_value = dot(inputs, gate_here)
            upward = dot(inputs, up_here)
            hidden.append((jax.nn.silu(gate_value) * upward).astype(BF16))
        return hidden

    for copy in loads[:3]:
        copy.wait()
    (hidden,) = swiglu(normed[...], [(sgate[...], sup[...])])
    shared_part = dot(hidden, sdown[...]).astype(BF16)
    for side_of in range(cores):
        shared_send[side_of] = shared_part[:, side_of * half : (side_of + 1) * half]
    pair = pltpu.make_async_remote_copy(
        src_ref=shared_send.at[other], dst_ref=shared_recv, send_sem=pair_send.at[0], recv_sem=pair_recv.at[0],
        device_id={"tp": other}, device_id_type=MESH,
    )
    pair.start()

    small[3].wait()
    small[4].wait()
    weights = weight[...]
    weight_t = functools.reduce(jnp.add, [jnp.where(hit, weights[k : k + 1, :], 0.0) for k, hit in enumerate(hits)])
    high = weight_t.astype(BF16)
    low = (weight_t - high.astype(F32)).astype(BF16)
    eye = (iota((local_tokens, local_tokens), 0) == iota((local_tokens, local_tokens), 1)).astype(F32).astype(BF16)
    turned = [
        lax.dot_general(eye, part, (((1,), (1,)), ((), ())), preferred_element_type=F32).astype(BF16)
        for part in (high, low, rank_t.astype(BF16))
    ]
    columns = experts * cores * thin
    expand = (iota((experts, columns), 0) == iota((experts, columns), 1) // (cores * thin)).astype(F32).astype(BF16)
    spread = dot(jnp.concatenate(turned, axis=0), expand)
    col = iota((local_tokens, columns), 1)
    slot_base = ((col // thin) % cores * chunks).astype(F32)
    q_col = col % thin
    for j in range(chunks):
        here = spread[2 * local_tokens :] == slot_base + j
        for part in range(2):
            value = jnp.where(here, spread[part * local_tokens : (part + 1) * local_tokens], 0.0)
            for q in range(thin):
                picks[j, pl.ds((part * thin + q) * local_tokens, local_tokens)] = jnp.where(
                    q_col == q, value, 0.0
                ).astype(BF16)

    pair.wait()
    for q in range(thin):
        lanes = slice(q * LANES, (q + 1) * LANES)
        total = shared_send[c][:, lanes].astype(F32) + shared_recv[:, lanes].astype(F32)
        shared_half[pl.ds(q * local_tokens, local_tokens)] = total.astype(BF16).astype(F32)

    for copy in loads[3:]:
        copy.wait()
    for copy in pushes:
        copy.wait()

    to_rows = one_hot_to_rows(wide, wide)
    per_back = 2 * LANES // thin
    to_thin = one_hot_to_blocks(per_back, thin)

    def give_back(j, offset, core):
        to = peer(offset)
        return pltpu.make_async_remote_copy(
            src_ref=tx2.at[j, core, to], dst_ref=rx2.at[j, ep * cores + c], send_sem=send2_sem.at[j], recv_sem=recv2_sem.at[j],
            device_id={"ep": to, "tp": core}, device_id_type=MESH,
        )

    partner_back = []
    for j in range(chunks):
        arrived = rx.at[j, pl.ds(0, experts - 1)]
        pltpu.make_async_copy(arrived, arrived, recv_sem.at[j]).wait()
        for b in range(experts // per_block):
            block = rx[j, pl.ds(b * per_block, per_block)].reshape(per_block * wide, LANES)
            sorted_rows = dot(to_rows, block).astype(BF16)
            for q in range(wide):
                rows[pl.ds(b * per_block, per_block), q * LANES : (q + 1) * LANES] = sorted_rows[
                    q * per_block : (q + 1) * per_block
                ]
        hidden = swiglu(rows[...], [(gate[h], up[h]) for h in range(cores)])
        result = functools.reduce(jnp.add, [dot(hidden[h], down[h]) for h in range(cores)]).astype(BF16)
        for b in range(experts // per_back):
            part = result[b * per_back : (b + 1) * per_back]
            for core in range(cores):
                stacked = jnp.concatenate(
                    [part[:, core * half + q * LANES : core * half + (q + 1) * LANES] for q in range(thin)], axis=0
                )
                tx2[j, core, pl.ds(b * per_back, per_back)] = (
                    dot(to_thin, stacked).astype(BF16).reshape(per_back, thin, LANES)
                )
        for offset in order:
            for core in range(cores):
                give_back(j, offset, core).start()
        back = pltpu.make_async_remote_copy(
            src_ref=tx2.at[j, other, ep], dst_ref=rx2.at[j, ep * cores + c], send_sem=send2_sem.at[j], recv_sem=recv2_sem.at[j],
            device_id={"tp": other}, device_id_type=MESH,
        )
        back.start()
        rx2[j, ep * cores + c] = tx2[j, c, ep]

    total = shared_half[...]
    for j in range(chunks):
        arrived = rx2.at[j, pl.ds(0, experts * cores - 1)]
        pltpu.make_async_copy(arrived, arrived, recv2_sem.at[j]).wait()
        summed = dot(picks[j], rx2[j].reshape(experts * cores * thin, LANES))
        total = total + summed[: thin * local_tokens] + summed[thin * local_tokens :]
    squares = total * total
    mine = functools.reduce(jnp.add, [squares[q * local_tokens : (q + 1) * local_tokens] for q in range(thin)])
    mine = jnp.broadcast_to(jnp.sum(mine, axis=1, keepdims=True), (local_tokens, LANES))
    sq_send[...] = mine
    pair = pltpu.make_async_remote_copy(
        src_ref=sq_send, dst_ref=sq_recv, send_sem=pair_send.at[1], recv_sem=pair_recv.at[1],
        device_id={"tp": other}, device_id_type=MESH,
    )
    pair.start()
    for j in range(chunks):
        sent = tx.at[j, pl.ds(0, experts - 1)]
        pltpu.make_async_copy(sent, sent, send_sem.at[j]).wait()
        sent = rx2.at[j, pl.ds(0, experts * cores - 1)]
        pltpu.make_async_copy(sent, sent, send2_sem.at[j]).wait()
    pair.wait()
    scale = lax.rsqrt((mine + sq_recv[...]) / width + EPSILON)
    gains = out_gain[...].astype(F32)
    for q in range(thin):
        lanes = slice(q * LANES, (q + 1) * LANES)
        out_ref[:, lanes] = (total[q * local_tokens : (q + 1) * local_tokens] * scale * gains[q : q + 1, :]).astype(BF16)


def body(tokens, in_gain, route_expert, route_weight, gate_weight, up_weight, down_weight, shared_gate, shared_up, shared_down, out_gain):
    experts, cores = lax.axis_size("ep"), lax.axis_size("tp")
    local_tokens, width = tokens.shape
    top_count = route_expert.shape[1]
    slots = max(2, (local_tokens * top_count * 4 + 3 * experts - 1) // (3 * experts))
    chunks = slots // cores
    half = width // cores
    wide, thin = width // LANES, half // LANES
    hidden = gate_weight.shape[2]
    any_spec = pl.BlockSpec(memory_space=pl.ANY)
    vmem, dma = pltpu.VMEM, pltpu.SemaphoreType.DMA
    scratch = [
        vmem((local_tokens, width), BF16), vmem((wide, LANES), BF16), vmem((top_count, local_tokens), jnp.int32),
        vmem((top_count, local_tokens), F32), vmem((thin, LANES), BF16),
        vmem((cores, width, hidden), BF16), vmem((cores, width, hidden), BF16), vmem((cores, hidden, width), BF16),
        vmem((width, hidden), BF16), vmem((width, hidden), BF16), vmem((hidden, width), BF16),
        vmem((local_tokens, width), BF16),
        vmem((chunks, experts, wide, LANES), BF16), vmem((chunks, experts, wide, LANES), BF16),
        vmem((experts, width), BF16),
        vmem((chunks, cores, experts, thin, LANES), BF16), vmem((chunks, experts * cores, thin, LANES), BF16),
        vmem((chunks, 2 * thin * local_tokens, experts * cores * thin), BF16),
        vmem((cores, local_tokens, half), BF16), vmem((local_tokens, half), BF16), vmem((thin * local_tokens, LANES), F32),
        vmem((local_tokens, LANES), F32), vmem((local_tokens, LANES), F32),
        dma((5,)), dma((6,)), dma((3,)), dma((3,)), dma((chunks,)), dma((chunks,)), dma((chunks,)), dma((chunks,)),
        dma((2,)), dma((2,)), pltpu.SemaphoreType.REGULAR, pltpu.SemaphoreType.REGULAR, pltpu.SemaphoreType.REGULAR,
    ]
    return pl.pallas_call(
        functools.partial(kernel, experts, cores, slots),
        out_shape=jax.ShapeDtypeStruct((local_tokens, half), BF16),
        in_specs=[any_spec] * 11,
        out_specs=pl.BlockSpec(memory_space=pltpu.VMEM),
        scratch_shapes=scratch,
        compiler_params=pltpu.CompilerParams(collective_id=0, has_side_effects=True, vmem_limit_bytes=60 * 1024 * 1024),
    )(
        tokens, in_gain.reshape(wide, LANES), route_expert.T, route_weight.T, gate_weight, up_weight, down_weight,
        shared_gate, shared_up, shared_down, out_gain.reshape(thin, LANES),
    )


def solution(mesh):
    return jax.shard_map(
        body,
        mesh=mesh,
        in_specs=(
            P(("grp", "ep"), None),
            P(),
            P(("grp", "ep"), None),
            P(("grp", "ep"), None),
            P("ep", None, "tp"),
            P("ep", None, "tp"),
            P("ep", "tp", None),
            P(None, "tp"),
            P(None, "tp"),
            P("tp", None),
            P("tp"),
        ),
        out_specs=P(("grp", "ep"), "tp"),
        check_vma=False,
    )
```

```python
import functools
import math

import jax
import jax.numpy as jnp
from jax import lax
from jax.experimental import pallas as pl
from jax.experimental.pallas import tpu as pltpu
from jax.sharding import PartitionSpec as P

EPSILON = 1e-06
BF16 = jnp.bfloat16
F32 = jnp.float32
LANES = 128
MESH = pl.DeviceIdType.MESH


def far_first(side):
    def reach(step):
        return min(step, side - step)

    offsets = [(dx, dy) for dy in range(side) for dx in range(side) if dx or dy]
    return sorted(offsets, key=lambda o: -(reach(o[0]) + reach(o[1])))


def dot(a, b):
    return jnp.dot(a, b, preferred_element_type=F32)


def iota(shape, dim):
    return lax.broadcasted_iota(jnp.int32, shape, dim)


def one_hot_to_rows(blocks, per_row):
    size = blocks * per_row
    row, col = iota((size, size), 0), iota((size, size), 1)
    return (col == (row % blocks) * per_row + row // blocks).astype(F32).astype(BF16)


def one_hot_to_blocks(blocks, per_row):
    size = blocks * per_row
    row, col = iota((size, size), 0), iota((size, size), 1)
    return (col == (row % per_row) * blocks + row // per_row).astype(F32).astype(BF16)


def kernel(
    experts, cores, slots,
    tokens_hbm, in_gain_hbm, route_hbm, weight_hbm, gate_hbm, up_hbm, down_hbm, sgate_hbm, sup_hbm, sdown_hbm, out_gain_hbm,
    out_ref,
    tokens, in_gain, route, weight, out_gain, gate, up, down, sgate, sup, sdown,
    normed, tx, rx, rows, tx2, rx2, picks, shared_send, shared_recv, shared_half, sq_send, sq_recv,
    small_sem, weight_sem, push_send, push_recv, send_sem, recv_sem, send2_sem, recv2_sem, pair_send, pair_recv, pair_sem,
):
    ep, c = lax.axis_index("ep"), lax.axis_index("tp")
    other = 1 - c
    side = math.isqrt(experts)
    here_x, here_y = lax.rem(ep, side), lax.div(ep, side)
    local_tokens, width = tokens.shape
    half = width // cores
    chunks = slots // cores
    wide = width // LANES
    thin = half // LANES
    order = far_first(side)

    def peer(offset):
        return lax.rem(here_y + offset[1], side) * side + lax.rem(here_x + offset[0], side)

    small = [
        pltpu.make_async_copy(src, dst, small_sem.at[i])
        for i, (src, dst) in enumerate(
            [(route_hbm, route), (tokens_hbm, tokens), (in_gain_hbm, in_gain), (weight_hbm, weight), (out_gain_hbm, out_gain)]
        )
    ]
    for copy in small:
        copy.start()
    barrier = pltpu.get_barrier_semaphore()

    for offset in order:
        pl.semaphore_signal(barrier, inc=1, device_id={"ep": peer(offset)}, device_id_type=MESH)
    pl.semaphore_signal(barrier, inc=1, device_id={"tp": other}, device_id_type=MESH)
    loads = [
        pltpu.make_async_copy(src, dst, weight_sem.at[i])
        for i, (src, dst) in enumerate(
            [
                (sgate_hbm, sgate), (sup_hbm, sup), (sdown_hbm, sdown),
                (gate_hbm.at[0], gate.at[0]), (up_hbm.at[0], up.at[0]), (down_hbm.at[0], down.at[0]),
            ]
        )
    ]
    for copy in loads:
        copy.start()

    small[0].wait()
    names = route[...]
    expert_row = iota((experts, local_tokens), 0)
    hits = [names[k : k + 1, :] == expert_row for k in range(names.shape[0])]
    chosen = functools.reduce(jnp.logical_or, hits)
    earlier = (iota((local_tokens, local_tokens), 0) < iota((local_tokens, local_tokens), 1)).astype(F32).astype(BF16)
    rank_t = jnp.where(chosen, dot(chosen.astype(F32).astype(BF16), earlier), -1.0)

    small[1].wait()
    small[2].wait()
    floats = tokens[...].astype(F32)
    scale = lax.rsqrt(jnp.mean(floats * floats, axis=1, keepdims=True) + EPSILON)
    gains = in_gain[...].astype(F32)
    for q in range(wide):
        lanes = slice(q * LANES, (q + 1) * LANES)
        normed[:, lanes] = (floats[:, lanes] * scale * gains[q : q + 1, :]).astype(BF16)

    to_blocks = one_hot_to_blocks(wide, wide)
    per_block = wide
    first_slot = (c * chunks).astype(F32)
    for j in range(chunks):
        pick = (rank_t == first_slot + j).astype(F32).astype(BF16)
        picked = dot(pick, normed[...]).astype(BF16)
        for b in range(experts // per_block):
            part = picked[b * per_block : (b + 1) * per_block]
            stacked = jnp.concatenate([part[:, q * LANES : (q + 1) * LANES] for q in range(wide)], axis=0)
            tx[j, pl.ds(b * per_block, per_block)] = (
                dot(to_blocks, stacked).astype(BF16).reshape(per_block, wide, LANES)
            )
        rx[j, ep] = tx[j, ep]

    def dispatch(j, to):
        return pltpu.make_async_remote_copy(
            src_ref=tx.at[j, to], dst_ref=rx.at[j, ep], send_sem=send_sem.at[j], recv_sem=recv_sem.at[j],
            device_id={"ep": to}, device_id_type=MESH,
        )

    pushes = [
        pltpu.make_async_remote_copy(
            src_ref=src.at[0], dst_ref=dst.at[1], send_sem=push_send.at[i], recv_sem=push_recv.at[i],
            device_id={"tp": other}, device_id_type=MESH,
        )
        for i, (src, dst) in enumerate([(gate_hbm, gate), (up_hbm, up), (down_hbm, down)])
    ]

    @pl.when(c == 1)
    def _():
        pl.semaphore_wait(barrier, experts)
        pl.semaphore_signal(pair_sem, inc=1, device_id={"tp": 0}, device_id_type=MESH)

    @pl.when(c == 0)
    def _():
        pl.semaphore_wait(pair_sem, 1)
        for copy in pushes:
            copy.start()
        pl.semaphore_wait(barrier, experts)
        pl.semaphore_signal(pair_sem, inc=1, device_id={"tp": 1}, device_id_type=MESH)

    for j in range(chunks):
        for offset in order:
            dispatch(j, peer(offset)).start()

    @pl.when(c == 1)
    def _():
        for copy in pushes:
            copy.start()

    def swiglu(inputs, pairs):
        hidden = []
        for gate_here, up_here in pairs:
            gate_value = dot(inputs, gate_here)
            upward = dot(inputs, up_here)
            hidden.append((jax.nn.silu(gate_value) * upward).astype(BF16))
        return hidden

    for copy in loads[:3]:
        copy.wait()
    (hidden,) = swiglu(normed[...], [(sgate[...], sup[...])])
    shared_part = dot(hidden, sdown[...]).astype(BF16)
    for side_of in range(cores):
        shared_send[side_of] = shared_part[:, side_of * half : (side_of + 1) * half]
    pair = pltpu.make_async_remote_copy(
        src_ref=shared_send.at[other], dst_ref=shared_recv, send_sem=pair_send.at[0], recv_sem=pair_recv.at[0],
        device_id={"tp": other}, device_id_type=MESH,
    )
    pair.start()

    small[3].wait()
    small[4].wait()
    weights = weight[...]
    weight_t = functools.reduce(jnp.add, [jnp.where(hit, weights[k : k + 1, :], 0.0) for k, hit in enumerate(hits)])
    high = weight_t.astype(BF16)
    low = (weight_t - high.astype(F32)).astype(BF16)
    eye = (iota((local_tokens, local_tokens), 0) == iota((local_tokens, local_tokens), 1)).astype(F32).astype(BF16)
    turned = [
        lax.dot_general(eye, part, (((1,), (1,)), ((), ())), preferred_element_type=F32).astype(BF16)
        for part in (high, low, rank_t.astype(BF16))
    ]
    columns = experts * cores * thin
    expand = (iota((experts, columns), 0) == iota((experts, columns), 1) // (cores * thin)).astype(F32).astype(BF16)
    spread = dot(jnp.concatenate(turned, axis=0), expand)
    col = iota((local_tokens, columns), 1)
    slot_base = ((col // thin) % cores * chunks).astype(F32)
    q_col = col % thin
    for j in range(chunks):
        here = spread[2 * local_tokens :] == slot_base + j
        for part in range(2):
            value = jnp.where(here, spread[part * local_tokens : (part + 1) * local_tokens], 0.0)
            for q in range(thin):
                picks[j, pl.ds((part * thin + q) * local_tokens, local_tokens)] = jnp.where(
                    q_col == q, value, 0.0
                ).astype(BF16)

    pair.wait()
    for q in range(thin):
        lanes = slice(q * LANES, (q + 1) * LANES)
        total = shared_send[c][:, lanes].astype(F32) + shared_recv[:, lanes].astype(F32)
        shared_half[pl.ds(q * local_tokens, local_tokens)] = total.astype(BF16).astype(F32)

    for copy in loads[3:]:
        copy.wait()
    for copy in pushes:
        copy.wait()

    to_rows = one_hot_to_rows(wide, wide)
    per_back = 2 * LANES // thin
    to_thin = one_hot_to_blocks(per_back, thin)

    def give_back(j, offset, core):
        to = peer(offset)
        return pltpu.make_async_remote_copy(
            src_ref=tx2.at[j, core, to], dst_ref=rx2.at[j, ep * cores + c], send_sem=send2_sem.at[j], recv_sem=recv2_sem.at[j],
            device_id={"ep": to, "tp": core}, device_id_type=MESH,
        )

    partner_back = []
    for j in range(chunks):
        arrived = rx.at[j, pl.ds(0, experts - 1)]
        pltpu.make_async_copy(arrived, arrived, recv_sem.at[j]).wait()
        for b in range(experts // per_block):
            block = rx[j, pl.ds(b * per_block, per_block)].reshape(per_block * wide, LANES)
            sorted_rows = dot(to_rows, block).astype(BF16)
            for q in range(wide):
                rows[pl.ds(b * per_block, per_block), q * LANES : (q + 1) * LANES] = sorted_rows[
                    q * per_block : (q + 1) * per_block
                ]
        hidden = swiglu(rows[...], [(gate[h], up[h]) for h in range(cores)])
        result = functools.reduce(jnp.add, [dot(hidden[h], down[h]) for h in range(cores)]).astype(BF16)
        for b in range(experts // per_back):
            part = result[b * per_back : (b + 1) * per_back]
            for core in range(cores):
                stacked = jnp.concatenate(
                    [part[:, core * half + q * LANES : core * half + (q + 1) * LANES] for q in range(thin)], axis=0
                )
                tx2[j, core, pl.ds(b * per_back, per_back)] = (
                    dot(to_thin, stacked).astype(BF16).reshape(per_back, thin, LANES)
                )
        for offset in order:
            give_back(j, offset, c).start()
        if j == 0:

            @pl.when(c == 1)
            def _():
                pl.semaphore_wait(pair_sem, 1)

        for offset in order:
            give_back(j, offset, other).start()
        back = pltpu.make_async_remote_copy(
            src_ref=tx2.at[j, other, ep], dst_ref=rx2.at[j, ep * cores + c], send_sem=send2_sem.at[j], recv_sem=recv2_sem.at[j],
            device_id={"tp": other}, device_id_type=MESH,
        )
        back.start()
        rx2[j, ep * cores + c] = tx2[j, c, ep]

    total = shared_half[...]
    for j in range(chunks):
        arrived = rx2.at[j, pl.ds(0, experts * cores - 1)]
        pltpu.make_async_copy(arrived, arrived, recv2_sem.at[j]).wait()
        summed = dot(picks[j], rx2[j].reshape(experts * cores * thin, LANES))
        total = total + summed[: thin * local_tokens] + summed[thin * local_tokens :]
    squares = total * total
    mine = functools.reduce(jnp.add, [squares[q * local_tokens : (q + 1) * local_tokens] for q in range(thin)])
    mine = jnp.broadcast_to(jnp.sum(mine, axis=1, keepdims=True), (local_tokens, LANES))
    sq_send[...] = mine
    pair = pltpu.make_async_remote_copy(
        src_ref=sq_send, dst_ref=sq_recv, send_sem=pair_send.at[1], recv_sem=pair_recv.at[1],
        device_id={"tp": other}, device_id_type=MESH,
    )
    pair.start()
    for j in range(chunks):
        sent = tx.at[j, pl.ds(0, experts - 1)]
        pltpu.make_async_copy(sent, sent, send_sem.at[j]).wait()
        sent = rx2.at[j, pl.ds(0, experts * cores - 1)]
        pltpu.make_async_copy(sent, sent, send2_sem.at[j]).wait()
    pair.wait()
    scale = lax.rsqrt((mine + sq_recv[...]) / width + EPSILON)
    gains = out_gain[...].astype(F32)
    for q in range(thin):
        lanes = slice(q * LANES, (q + 1) * LANES)
        out_ref[:, lanes] = (total[q * local_tokens : (q + 1) * local_tokens] * scale * gains[q : q + 1, :]).astype(BF16)


def body(tokens, in_gain, route_expert, route_weight, gate_weight, up_weight, down_weight, shared_gate, shared_up, shared_down, out_gain):
    experts, cores = lax.axis_size("ep"), lax.axis_size("tp")
    local_tokens, width = tokens.shape
    top_count = route_expert.shape[1]
    slots = max(2, (local_tokens * top_count * 4 + 3 * experts - 1) // (3 * experts))
    chunks = slots // cores
    half = width // cores
    wide, thin = width // LANES, half // LANES
    hidden = gate_weight.shape[2]
    any_spec = pl.BlockSpec(memory_space=pl.ANY)
    vmem, dma = pltpu.VMEM, pltpu.SemaphoreType.DMA
    scratch = [
        vmem((local_tokens, width), BF16), vmem((wide, LANES), BF16), vmem((top_count, local_tokens), jnp.int32),
        vmem((top_count, local_tokens), F32), vmem((thin, LANES), BF16),
        vmem((cores, width, hidden), BF16), vmem((cores, width, hidden), BF16), vmem((cores, hidden, width), BF16),
        vmem((width, hidden), BF16), vmem((width, hidden), BF16), vmem((hidden, width), BF16),
        vmem((local_tokens, width), BF16),
        vmem((chunks, experts, wide, LANES), BF16), vmem((chunks, experts, wide, LANES), BF16),
        vmem((experts, width), BF16),
        vmem((chunks, cores, experts, thin, LANES), BF16), vmem((chunks, experts * cores, thin, LANES), BF16),
        vmem((chunks, 2 * thin * local_tokens, experts * cores * thin), BF16),
        vmem((cores, local_tokens, half), BF16), vmem((local_tokens, half), BF16), vmem((thin * local_tokens, LANES), F32),
        vmem((local_tokens, LANES), F32), vmem((local_tokens, LANES), F32),
        dma((5,)), dma((6,)), dma((3,)), dma((3,)), dma((chunks,)), dma((chunks,)), dma((chunks,)), dma((chunks,)),
        dma((2,)), dma((2,)), pltpu.SemaphoreType.REGULAR,
    ]
    return pl.pallas_call(
        functools.partial(kernel, experts, cores, slots),
        out_shape=jax.ShapeDtypeStruct((local_tokens, half), BF16),
        in_specs=[any_spec] * 11,
        out_specs=pl.BlockSpec(memory_space=pltpu.VMEM),
        scratch_shapes=scratch,
        compiler_params=pltpu.CompilerParams(collective_id=0, has_side_effects=True, vmem_limit_bytes=60 * 1024 * 1024),
    )(
        tokens, in_gain.reshape(wide, LANES), route_expert.T, route_weight.T, gate_weight, up_weight, down_weight,
        shared_gate, shared_up, shared_down, out_gain.reshape(thin, LANES),
    )


def solution(mesh):
    return jax.shard_map(
        body,
        mesh=mesh,
        in_specs=(
            P(("grp", "ep"), None),
            P(),
            P(("grp", "ep"), None),
            P(("grp", "ep"), None),
            P("ep", None, "tp"),
            P("ep", None, "tp"),
            P("ep", "tp", None),
            P(None, "tp"),
            P(None, "tp"),
            P("tp", None),
            P("tp"),
        ),
        out_specs=P(("grp", "ep"), "tp"),
        check_vma=False,
    )
```

```python
import functools
import math

import jax
import jax.numpy as jnp
from jax import lax
from jax.experimental import pallas as pl
from jax.experimental.pallas import tpu as pltpu
from jax.sharding import PartitionSpec as P

EPSILON = 1e-06
BF16 = jnp.bfloat16
F32 = jnp.float32
LANES = 128
MESH = pl.DeviceIdType.MESH


def far_first(side):
    def reach(step):
        return min(step, side - step)

    offsets = [(dx, dy) for dy in range(side) for dx in range(side) if dx or dy]
    return sorted(offsets, key=lambda o: -(reach(o[0]) + reach(o[1])))


def dot(a, b):
    return jnp.dot(a, b, preferred_element_type=F32)


def iota(shape, dim):
    return lax.broadcasted_iota(jnp.int32, shape, dim)


def one_hot_to_rows(blocks, per_row):
    size = blocks * per_row
    row, col = iota((size, size), 0), iota((size, size), 1)
    return (col == (row % blocks) * per_row + row // blocks).astype(F32).astype(BF16)


def one_hot_to_blocks(blocks, per_row):
    size = blocks * per_row
    row, col = iota((size, size), 0), iota((size, size), 1)
    return (col == (row % per_row) * blocks + row // per_row).astype(F32).astype(BF16)


def kernel(
    experts, cores, slots,
    tokens_hbm, in_gain_hbm, route_hbm, weight_hbm, gate_hbm, up_hbm, down_hbm, sgate_hbm, sup_hbm, sdown_hbm, out_gain_hbm,
    out_ref,
    tokens, in_gain, route, weight, out_gain, gate, up, down, sgate, sup, sdown,
    normed, tx, rx, rows, tx2, rx2, picks, shared_send, shared_recv, shared_half, sq_send, sq_recv,
    small_sem, weight_sem, push_send, push_recv, send_sem, recv_sem, send2_sem, recv2_sem, pair_send, pair_recv, pair_sem,
):
    ep, c = lax.axis_index("ep"), lax.axis_index("tp")
    other = 1 - c
    side = math.isqrt(experts)
    here_x, here_y = lax.rem(ep, side), lax.div(ep, side)
    local_tokens, width = tokens.shape
    half = width // cores
    chunks = slots // cores
    wide = width // LANES
    thin = half // LANES
    order = far_first(side)
    is_root = ep == 0
    counts_partner = is_root == (c == 0)

    def peer(offset):
        return lax.rem(here_y + offset[1], side) * side + lax.rem(here_x + offset[0], side)

    small = [
        pltpu.make_async_copy(src, dst, small_sem.at[i])
        for i, (src, dst) in enumerate(
            [(route_hbm, route), (tokens_hbm, tokens), (in_gain_hbm, in_gain), (weight_hbm, weight), (out_gain_hbm, out_gain)]
        )
    ]
    for copy in small:
        copy.start()
    barrier = pltpu.get_barrier_semaphore()

    for offset in order:
        pl.semaphore_signal(barrier, inc=1, device_id={"ep": peer(offset)}, device_id_type=MESH)

    @pl.when(jnp.logical_not(counts_partner))
    def _():
        pl.semaphore_signal(barrier, inc=1, device_id={"tp": other}, device_id_type=MESH)

    loads = [
        pltpu.make_async_copy(src, dst, weight_sem.at[i])
        for i, (src, dst) in enumerate(
            [
                (sgate_hbm, sgate), (sup_hbm, sup), (sdown_hbm, sdown),
                (gate_hbm.at[0], gate.at[0]), (up_hbm.at[0], up.at[0]), (down_hbm.at[0], down.at[0]),
            ]
        )
    ]
    for copy in loads:
        copy.start()

    small[0].wait()
    names = route[...]
    expert_row = iota((experts, local_tokens), 0)
    hits = [names[k : k + 1, :] == expert_row for k in range(names.shape[0])]
    chosen = functools.reduce(jnp.logical_or, hits)
    earlier = (iota((local_tokens, local_tokens), 0) < iota((local_tokens, local_tokens), 1)).astype(F32).astype(BF16)
    rank_t = jnp.where(chosen, dot(chosen.astype(F32).astype(BF16), earlier), -1.0)

    small[1].wait()
    small[2].wait()
    floats = tokens[...].astype(F32)
    scale = lax.rsqrt(jnp.mean(floats * floats, axis=1, keepdims=True) + EPSILON)
    gains = in_gain[...].astype(F32)
    for q in range(wide):
        lanes = slice(q * LANES, (q + 1) * LANES)
        normed[:, lanes] = (floats[:, lanes] * scale * gains[q : q + 1, :]).astype(BF16)

    to_blocks = one_hot_to_blocks(wide, wide)
    per_block = wide
    first_slot = (c * chunks).astype(F32)
    for j in range(chunks):
        pick = (rank_t == first_slot + j).astype(F32).astype(BF16)
        picked = dot(pick, normed[...]).astype(BF16)
        for b in range(experts // per_block):
            part = picked[b * per_block : (b + 1) * per_block]
            stacked = jnp.concatenate([part[:, q * LANES : (q + 1) * LANES] for q in range(wide)], axis=0)
            tx[j, pl.ds(b * per_block, per_block)] = (
                dot(to_blocks, stacked).astype(BF16).reshape(per_block, wide, LANES)
            )
        rx[j, ep] = tx[j, ep]

    def dispatch(j, to):
        return pltpu.make_async_remote_copy(
            src_ref=tx.at[j, to], dst_ref=rx.at[j, ep], send_sem=send_sem.at[j], recv_sem=recv_sem.at[j],
            device_id={"ep": to}, device_id_type=MESH,
        )

    pushes = [
        pltpu.make_async_remote_copy(
            src_ref=src.at[0], dst_ref=dst.at[1], send_sem=push_send.at[i], recv_sem=push_recv.at[i],
            device_id={"tp": other}, device_id_type=MESH,
        )
        for i, (src, dst) in enumerate([(gate_hbm, gate), (up_hbm, up), (down_hbm, down)])
    ]

    def tell_partner():
        pl.semaphore_signal(pair_sem, inc=1, device_id={"tp": other}, device_id_type=MESH)

    def push():
        for copy in pushes:
            copy.start()

    @pl.when(jnp.logical_and(c == 0, is_root))
    def _():
        pl.semaphore_wait(barrier, experts)
        tell_partner()
        push()

    @pl.when(jnp.logical_and(c == 0, jnp.logical_not(is_root)))
    def _():
        pl.semaphore_wait(pair_sem, 1)
        push()
        pl.semaphore_wait(barrier, experts - 1)
        tell_partner()

    @pl.when(jnp.logical_and(c == 1, is_root))
    def _():
        pl.semaphore_wait(barrier, experts - 1)

    @pl.when(jnp.logical_and(c == 1, jnp.logical_not(is_root)))
    def _():
        pl.semaphore_wait(barrier, experts)
        tell_partner()

    for j in range(chunks):
        for offset in order:
            dispatch(j, peer(offset)).start()

    @pl.when(jnp.logical_and(c == 1, is_root))
    def _():
        pl.semaphore_wait(pair_sem, 1)
        tell_partner()

    @pl.when(c == 1)
    def _():
        push()

    def swiglu(inputs, pairs):
        hidden = []
        for gate_here, up_here in pairs:
            gate_value = dot(inputs, gate_here)
            upward = dot(inputs, up_here)
            hidden.append((jax.nn.silu(gate_value) * upward).astype(BF16))
        return hidden

    for copy in loads[:3]:
        copy.wait()
    (hidden,) = swiglu(normed[...], [(sgate[...], sup[...])])
    shared_part = dot(hidden, sdown[...]).astype(BF16)
    for side_of in range(cores):
        shared_send[side_of] = shared_part[:, side_of * half : (side_of + 1) * half]
    pair = pltpu.make_async_remote_copy(
        src_ref=shared_send.at[other], dst_ref=shared_recv, send_sem=pair_send.at[0], recv_sem=pair_recv.at[0],
        device_id={"tp": other}, device_id_type=MESH,
    )
    pair.start()

    small[3].wait()
    small[4].wait()
    weights = weight[...]
    weight_t = functools.reduce(jnp.add, [jnp.where(hit, weights[k : k + 1, :], 0.0) for k, hit in enumerate(hits)])
    high = weight_t.astype(BF16)
    low = (weight_t - high.astype(F32)).astype(BF16)
    eye = (iota((local_tokens, local_tokens), 0) == iota((local_tokens, local_tokens), 1)).astype(F32).astype(BF16)
    turned = [
        lax.dot_general(eye, part, (((1,), (1,)), ((), ())), preferred_element_type=F32).astype(BF16)
        for part in (high, low, rank_t.astype(BF16))
    ]
    columns = experts * cores * thin
    expand = (iota((experts, columns), 0) == iota((experts, columns), 1) // (cores * thin)).astype(F32).astype(BF16)
    spread = dot(jnp.concatenate(turned, axis=0), expand)
    col = iota((local_tokens, columns), 1)
    slot_base = ((col // thin) % cores * chunks).astype(F32)
    q_col = col % thin
    for j in range(chunks):
        here = spread[2 * local_tokens :] == slot_base + j
        for part in range(2):
            value = jnp.where(here, spread[part * local_tokens : (part + 1) * local_tokens], 0.0)
            for q in range(thin):
                picks[j, pl.ds((part * thin + q) * local_tokens, local_tokens)] = jnp.where(
                    q_col == q, value, 0.0
                ).astype(BF16)

    pair.wait()
    for q in range(thin):
        lanes = slice(q * LANES, (q + 1) * LANES)
        total = shared_send[c][:, lanes].astype(F32) + shared_recv[:, lanes].astype(F32)
        shared_half[pl.ds(q * local_tokens, local_tokens)] = total.astype(BF16).astype(F32)

    for copy in loads[3:]:
        copy.wait()
    for copy in pushes:
        copy.wait()

    to_rows = one_hot_to_rows(wide, wide)
    per_back = 2 * LANES // thin
    to_thin = one_hot_to_blocks(per_back, thin)

    def give_back(j, offset, core):
        to = peer(offset)
        return pltpu.make_async_remote_copy(
            src_ref=tx2.at[j, core, to], dst_ref=rx2.at[j, ep * cores + c], send_sem=send2_sem.at[j], recv_sem=recv2_sem.at[j],
            device_id={"ep": to, "tp": core}, device_id_type=MESH,
        )

    def to_other_plane(j):
        for offset in order:
            give_back(j, offset, other).start()
        back = pltpu.make_async_remote_copy(
            src_ref=tx2.at[j, other, ep], dst_ref=rx2.at[j, ep * cores + c], send_sem=send2_sem.at[j], recv_sem=recv2_sem.at[j],
            device_id={"tp": other}, device_id_type=MESH,
        )
        back.start()

    for j in range(chunks):
        arrived = rx.at[j, pl.ds(0, experts - 1)]
        pltpu.make_async_copy(arrived, arrived, recv_sem.at[j]).wait()
        for b in range(experts // per_block):
            block = rx[j, pl.ds(b * per_block, per_block)].reshape(per_block * wide, LANES)
            sorted_rows = dot(to_rows, block).astype(BF16)
            for q in range(wide):
                rows[pl.ds(b * per_block, per_block), q * LANES : (q + 1) * LANES] = sorted_rows[
                    q * per_block : (q + 1) * per_block
                ]
        hidden = swiglu(rows[...], [(gate[h], up[h]) for h in range(cores)])
        result = functools.reduce(jnp.add, [dot(hidden[h], down[h]) for h in range(cores)]).astype(BF16)
        for b in range(experts // per_back):
            part = result[b * per_back : (b + 1) * per_back]
            for core in range(cores):
                stacked = jnp.concatenate(
                    [part[:, core * half + q * LANES : core * half + (q + 1) * LANES] for q in range(thin)], axis=0
                )
                tx2[j, core, pl.ds(b * per_back, per_back)] = (
                    dot(to_thin, stacked).astype(BF16).reshape(per_back, thin, LANES)
                )
        for offset in order:
            give_back(j, offset, c).start()
        rx2[j, ep * cores + c] = tx2[j, c, ep]
        if j == 0:

            @pl.when(jnp.logical_and(c == 0, is_root))
            def _():
                pl.semaphore_wait(pair_sem, 1)

        @pl.when(c == 0)
        def _():
            to_other_plane(j)

    @pl.when(jnp.logical_and(c == 1, jnp.logical_not(is_root)))
    def _():
        pl.semaphore_wait(pair_sem, 1)

    @pl.when(c == 1)
    def _():
        for j in range(chunks):
            to_other_plane(j)

    total = shared_half[...]
    for j in range(chunks):
        arrived = rx2.at[j, pl.ds(0, experts * cores - 1)]
        pltpu.make_async_copy(arrived, arrived, recv2_sem.at[j]).wait()
        summed = dot(picks[j], rx2[j].reshape(experts * cores * thin, LANES))
        total = total + summed[: thin * local_tokens] + summed[thin * local_tokens :]
    squares = total * total
    mine = functools.reduce(jnp.add, [squares[q * local_tokens : (q + 1) * local_tokens] for q in range(thin)])
    mine = jnp.broadcast_to(jnp.sum(mine, axis=1, keepdims=True), (local_tokens, LANES))
    sq_send[...] = mine
    pair = pltpu.make_async_remote_copy(
        src_ref=sq_send, dst_ref=sq_recv, send_sem=pair_send.at[1], recv_sem=pair_recv.at[1],
        device_id={"tp": other}, device_id_type=MESH,
    )
    pair.start()
    for j in range(chunks):
        sent = tx.at[j, pl.ds(0, experts - 1)]
        pltpu.make_async_copy(sent, sent, send_sem.at[j]).wait()
        sent = rx2.at[j, pl.ds(0, experts * cores - 1)]
        pltpu.make_async_copy(sent, sent, send2_sem.at[j]).wait()
    pair.wait()
    scale = lax.rsqrt((mine + sq_recv[...]) / width + EPSILON)
    gains = out_gain[...].astype(F32)
    for q in range(thin):
        lanes = slice(q * LANES, (q + 1) * LANES)
        out_ref[:, lanes] = (total[q * local_tokens : (q + 1) * local_tokens] * scale * gains[q : q + 1, :]).astype(BF16)


def body(tokens, in_gain, route_expert, route_weight, gate_weight, up_weight, down_weight, shared_gate, shared_up, shared_down, out_gain):
    experts, cores = lax.axis_size("ep"), lax.axis_size("tp")
    local_tokens, width = tokens.shape
    top_count = route_expert.shape[1]
    slots = max(2, (local_tokens * top_count * 4 + 3 * experts - 1) // (3 * experts))
    chunks = slots // cores
    half = width // cores
    wide, thin = width // LANES, half // LANES
    hidden = gate_weight.shape[2]
    any_spec = pl.BlockSpec(memory_space=pl.ANY)
    vmem, dma = pltpu.VMEM, pltpu.SemaphoreType.DMA
    scratch = [
        vmem((local_tokens, width), BF16), vmem((wide, LANES), BF16), vmem((top_count, local_tokens), jnp.int32),
        vmem((top_count, local_tokens), F32), vmem((thin, LANES), BF16),
        vmem((cores, width, hidden), BF16), vmem((cores, width, hidden), BF16), vmem((cores, hidden, width), BF16),
        vmem((width, hidden), BF16), vmem((width, hidden), BF16), vmem((hidden, width), BF16),
        vmem((local_tokens, width), BF16),
        vmem((chunks, experts, wide, LANES), BF16), vmem((chunks, experts, wide, LANES), BF16),
        vmem((experts, width), BF16),
        vmem((chunks, cores, experts, thin, LANES), BF16), vmem((chunks, experts * cores, thin, LANES), BF16),
        vmem((chunks, 2 * thin * local_tokens, experts * cores * thin), BF16),
        vmem((cores, local_tokens, half), BF16), vmem((local_tokens, half), BF16), vmem((thin * local_tokens, LANES), F32),
        vmem((local_tokens, LANES), F32), vmem((local_tokens, LANES), F32),
        dma((5,)), dma((6,)), dma((3,)), dma((3,)), dma((chunks,)), dma((chunks,)), dma((chunks,)), dma((chunks,)),
        dma((2,)), dma((2,)), pltpu.SemaphoreType.REGULAR,
    ]
    return pl.pallas_call(
        functools.partial(kernel, experts, cores, slots),
        out_shape=jax.ShapeDtypeStruct((local_tokens, half), BF16),
        in_specs=[any_spec] * 11,
        out_specs=pl.BlockSpec(memory_space=pltpu.VMEM),
        scratch_shapes=scratch,
        compiler_params=pltpu.CompilerParams(collective_id=0, has_side_effects=True, vmem_limit_bytes=60 * 1024 * 1024),
    )(
        tokens, in_gain.reshape(wide, LANES), route_expert.T, route_weight.T, gate_weight, up_weight, down_weight,
        shared_gate, shared_up, shared_down, out_gain.reshape(thin, LANES),
    )


def solution(mesh):
    return jax.shard_map(
        body,
        mesh=mesh,
        in_specs=(
            P(("grp", "ep"), None),
            P(),
            P(("grp", "ep"), None),
            P(("grp", "ep"), None),
            P("ep", None, "tp"),
            P("ep", None, "tp"),
            P("ep", "tp", None),
            P(None, "tp"),
            P(None, "tp"),
            P("tp", None),
            P("tp"),
        ),
        out_specs=P(("grp", "ep"), "tp"),
        check_vma=False,
    )
```

```python
import functools
import math

import jax
import jax.numpy as jnp
from jax import lax
from jax.experimental import pallas as pl
from jax.experimental.pallas import tpu as pltpu
from jax.sharding import PartitionSpec as P

EPSILON = 1e-06
BF16 = jnp.bfloat16
F32 = jnp.float32
LANES = 128
MESH = pl.DeviceIdType.MESH


def far_first(side):
    def reach(step):
        return min(step, side - step)

    offsets = [(dx, dy) for dy in range(side) for dx in range(side) if dx or dy]
    return sorted(offsets, key=lambda o: -(reach(o[0]) + reach(o[1])))


def dot(a, b):
    return jnp.dot(a, b, preferred_element_type=F32)


def iota(shape, dim):
    return lax.broadcasted_iota(jnp.int32, shape, dim)


def one_hot_to_rows(blocks, per_row):
    size = blocks * per_row
    row, col = iota((size, size), 0), iota((size, size), 1)
    return (col == (row % blocks) * per_row + row // blocks).astype(F32).astype(BF16)


def one_hot_to_blocks(blocks, per_row):
    size = blocks * per_row
    row, col = iota((size, size), 0), iota((size, size), 1)
    return (col == (row % per_row) * blocks + row // per_row).astype(F32).astype(BF16)


def kernel(
    experts, cores, slots,
    tokens_hbm, in_gain_hbm, route_hbm, weight_hbm, gate_hbm, up_hbm, down_hbm, sgate_hbm, sup_hbm, sdown_hbm, out_gain_hbm,
    out_ref,
    tokens, in_gain, route, weight, out_gain, gate, up, down, sgate, sup, sdown,
    normed, tx, rx, rows, tx2, rx2, picks, shared_send, shared_recv, shared_half, sq_send, sq_recv,
    small_sem, weight_sem, push_send, push_recv, send_sem, recv_sem, send2_sem, recv2_sem, forward_sem, pair_send, pair_recv, pair_sem, late_sem,
):
    ep, c = lax.axis_index("ep"), lax.axis_index("tp")
    other = 1 - c
    side = math.isqrt(experts)
    here_x, here_y = lax.rem(ep, side), lax.div(ep, side)
    local_tokens, width = tokens.shape
    half = width // cores
    chunks = slots // cores
    wide = width // LANES
    thin = half // LANES
    order = far_first(side)
    is_root = ep == 0
    is_late = jnp.logical_and(is_root, c == 0)
    is_mailbox = jnp.logical_and(is_root, c == 1)
    counts_partner = is_root == (c == 0)

    def peer(offset):
        return lax.rem(here_y + offset[1], side) * side + lax.rem(here_x + offset[0], side)

    small = [
        pltpu.make_async_copy(src, dst, small_sem.at[i])
        for i, (src, dst) in enumerate(
            [(route_hbm, route), (tokens_hbm, tokens), (in_gain_hbm, in_gain), (weight_hbm, weight), (out_gain_hbm, out_gain)]
        )
    ]
    for copy in small:
        copy.start()
    barrier = pltpu.get_barrier_semaphore()

    @pl.when(jnp.logical_not(is_late))
    def _():
        for offset in order:
            pl.semaphore_signal(barrier, inc=1, device_id={"ep": peer(offset)}, device_id_type=MESH)

    @pl.when(jnp.logical_not(counts_partner))
    def _():
        pl.semaphore_signal(barrier, inc=1, device_id={"tp": other}, device_id_type=MESH)

    loads = [
        pltpu.make_async_copy(src, dst, weight_sem.at[i])
        for i, (src, dst) in enumerate(
            [
                (sgate_hbm, sgate), (sup_hbm, sup), (sdown_hbm, sdown),
                (gate_hbm.at[0], gate.at[0]), (up_hbm.at[0], up.at[0]), (down_hbm.at[0], down.at[0]),
            ]
        )
    ]
    for copy in loads:
        copy.start()

    small[0].wait()
    names = route[...]
    expert_row = iota((experts, local_tokens), 0)
    hits = [names[k : k + 1, :] == expert_row for k in range(names.shape[0])]
    chosen = functools.reduce(jnp.logical_or, hits)
    earlier = (iota((local_tokens, local_tokens), 0) < iota((local_tokens, local_tokens), 1)).astype(F32).astype(BF16)
    rank_t = jnp.where(chosen, dot(chosen.astype(F32).astype(BF16), earlier), -1.0)

    small[1].wait()
    small[2].wait()
    floats = tokens[...].astype(F32)
    scale = lax.rsqrt(jnp.mean(floats * floats, axis=1, keepdims=True) + EPSILON)
    gains = in_gain[...].astype(F32)
    for q in range(wide):
        lanes = slice(q * LANES, (q + 1) * LANES)
        normed[:, lanes] = (floats[:, lanes] * scale * gains[q : q + 1, :]).astype(BF16)

    to_blocks = one_hot_to_blocks(wide, wide)
    per_block = wide
    first_slot = (c * chunks).astype(F32)
    for j in range(chunks):
        pick = (rank_t == first_slot + j).astype(F32).astype(BF16)
        picked = dot(pick, normed[...]).astype(BF16)
        for b in range(experts // per_block):
            part = picked[b * per_block : (b + 1) * per_block]
            stacked = jnp.concatenate([part[:, q * LANES : (q + 1) * LANES] for q in range(wide)], axis=0)
            tx[j, pl.ds(b * per_block, per_block)] = (
                dot(to_blocks, stacked).astype(BF16).reshape(per_block, wide, LANES)
            )
        rx[j, ep] = tx[j, ep]

    def dispatch(j, to):
        redirect = jnp.logical_and(to == 0, c == 0).astype(jnp.int32)
        return pltpu.make_async_remote_copy(
            src_ref=tx.at[j, to], dst_ref=rx.at[j, ep + redirect * experts], send_sem=send_sem.at[j],
            recv_sem=recv_sem.at[j + redirect * chunks], device_id={"ep": to, "tp": c + redirect}, device_id_type=MESH,
        )

    forwards = [
        pltpu.make_async_remote_copy(
            src_ref=rx.at[j, pl.ds(experts + 1, experts - 1)], dst_ref=rx.at[j, pl.ds(1, experts - 1)],
            send_sem=forward_sem.at[j], recv_sem=recv_sem.at[j], device_id={"tp": 0}, device_id_type=MESH,
        )
        for j in range(chunks)
    ]

    pushes = [
        pltpu.make_async_remote_copy(
            src_ref=src.at[0], dst_ref=dst.at[1], send_sem=push_send.at[i], recv_sem=push_recv.at[i],
            device_id={"tp": other}, device_id_type=MESH,
        )
        for i, (src, dst) in enumerate([(gate_hbm, gate), (up_hbm, up), (down_hbm, down)])
    ]

    def tell_partner():
        pl.semaphore_signal(pair_sem, inc=1, device_id={"tp": other}, device_id_type=MESH)

    def push():
        for copy in pushes:
            copy.start()

    @pl.when(jnp.logical_and(c == 0, is_root))
    def _():
        pl.semaphore_wait(barrier, experts)
        tell_partner()
        push()

    @pl.when(jnp.logical_and(c == 0, jnp.logical_not(is_root)))
    def _():
        pl.semaphore_wait(pair_sem, 1)
        push()
        pl.semaphore_wait(barrier, experts - 2)
        tell_partner()

    @pl.when(jnp.logical_and(c == 1, is_root))
    def _():
        pl.semaphore_wait(barrier, experts - 1)

    @pl.when(jnp.logical_and(c == 1, jnp.logical_not(is_root)))
    def _():
        pl.semaphore_wait(barrier, experts)
        tell_partner()

    for j in range(chunks):
        for offset in order:
            dispatch(j, peer(offset)).start()
        if j == 0:

            @pl.when(is_late)
            def _():
                for offset in order:
                    pl.semaphore_signal(late_sem, inc=1, device_id={"ep": peer(offset)}, device_id_type=MESH)

    @pl.when(jnp.logical_and(c == 1, is_root))
    def _():
        pl.semaphore_wait(pair_sem, 1)
        tell_partner()

    @pl.when(c == 1)
    def _():
        push()

    def swiglu(inputs, pairs):
        hidden = []
        for gate_here, up_here in pairs:
            gate_value = dot(inputs, gate_here)
            upward = dot(inputs, up_here)
            hidden.append((jax.nn.silu(gate_value) * upward).astype(BF16))
        return hidden

    for copy in loads[:3]:
        copy.wait()
    (hidden,) = swiglu(normed[...], [(sgate[...], sup[...])])
    shared_part = dot(hidden, sdown[...]).astype(BF16)
    for side_of in range(cores):
        shared_send[side_of] = shared_part[:, side_of * half : (side_of + 1) * half]
    pair = pltpu.make_async_remote_copy(
        src_ref=shared_send.at[other], dst_ref=shared_recv, send_sem=pair_send.at[0], recv_sem=pair_recv.at[0],
        device_id={"tp": other}, device_id_type=MESH,
    )
    pair.start()

    small[3].wait()
    small[4].wait()
    weights = weight[...]
    weight_t = functools.reduce(jnp.add, [jnp.where(hit, weights[k : k + 1, :], 0.0) for k, hit in enumerate(hits)])
    high = weight_t.astype(BF16)
    low = (weight_t - high.astype(F32)).astype(BF16)
    eye = (iota((local_tokens, local_tokens), 0) == iota((local_tokens, local_tokens), 1)).astype(F32).astype(BF16)
    turned = [
        lax.dot_general(eye, part, (((1,), (1,)), ((), ())), preferred_element_type=F32).astype(BF16)
        for part in (high, low, rank_t.astype(BF16))
    ]
    columns = experts * cores * thin
    expand = (iota((experts, columns), 0) == iota((experts, columns), 1) // (cores * thin)).astype(F32).astype(BF16)
    spread = dot(jnp.concatenate(turned, axis=0), expand)
    col = iota((local_tokens, columns), 1)
    slot_base = ((col // thin) % cores * chunks).astype(F32)
    q_col = col % thin
    for j in range(chunks):
        here = spread[2 * local_tokens :] == slot_base + j
        for part in range(2):
            value = jnp.where(here, spread[part * local_tokens : (part + 1) * local_tokens], 0.0)
            for q in range(thin):
                picks[j, pl.ds((part * thin + q) * local_tokens, local_tokens)] = jnp.where(
                    q_col == q, value, 0.0
                ).astype(BF16)

    pair.wait()
    for q in range(thin):
        lanes = slice(q * LANES, (q + 1) * LANES)
        total = shared_send[c][:, lanes].astype(F32) + shared_recv[:, lanes].astype(F32)
        shared_half[pl.ds(q * local_tokens, local_tokens)] = total.astype(BF16).astype(F32)

    @pl.when(jnp.logical_and(c == 0, jnp.logical_not(is_root)))
    def _():
        pl.semaphore_wait(late_sem, 1)
        pl.semaphore_signal(late_sem, inc=1, device_id={"tp": 1}, device_id_type=MESH)

    def forward(j):
        @pl.when(is_mailbox)
        def _():
            arrived = rx.at[j, pl.ds(experts + 1, experts - 1)]
            pltpu.make_async_copy(arrived, arrived, recv_sem.at[chunks + j]).wait()
            forwards[j].start()

    forward(0)
    for copy in loads[3:]:
        copy.wait()
    for copy in pushes:
        copy.wait()

    to_rows = one_hot_to_rows(wide, wide)
    per_back = 2 * LANES // thin
    to_thin = one_hot_to_blocks(per_back, thin)

    def give_back(j, offset, core):
        to = peer(offset)
        return pltpu.make_async_remote_copy(
            src_ref=tx2.at[j, core, to], dst_ref=rx2.at[j, ep * cores + c], send_sem=send2_sem.at[j], recv_sem=recv2_sem.at[j],
            device_id={"ep": to, "tp": core}, device_id_type=MESH,
        )

    def to_other_plane(j):
        for offset in order:
            give_back(j, offset, other).start()
        back = pltpu.make_async_remote_copy(
            src_ref=tx2.at[j, other, ep], dst_ref=rx2.at[j, ep * cores + c], send_sem=send2_sem.at[j], recv_sem=recv2_sem.at[j],
            device_id={"tp": other}, device_id_type=MESH,
        )
        back.start()

    for j in range(chunks):
        if j:
            forward(j)
        arrived = rx.at[j, pl.ds(0, experts - 1)]
        pltpu.make_async_copy(arrived, arrived, recv_sem.at[j]).wait()
        for b in range(experts // per_block):
            block = rx[j, pl.ds(b * per_block, per_block)].reshape(per_block * wide, LANES)
            sorted_rows = dot(to_rows, block).astype(BF16)
            for q in range(wide):
                rows[pl.ds(b * per_block, per_block), q * LANES : (q + 1) * LANES] = sorted_rows[
                    q * per_block : (q + 1) * per_block
                ]
        hidden = swiglu(rows[...], [(gate[h], up[h]) for h in range(cores)])
        result = functools.reduce(jnp.add, [dot(hidden[h], down[h]) for h in range(cores)]).astype(BF16)
        for b in range(experts // per_back):
            part = result[b * per_back : (b + 1) * per_back]
            for core in range(cores):
                stacked = jnp.concatenate(
                    [part[:, core * half + q * LANES : core * half + (q + 1) * LANES] for q in range(thin)], axis=0
                )
                tx2[j, core, pl.ds(b * per_back, per_back)] = (
                    dot(to_thin, stacked).astype(BF16).reshape(per_back, thin, LANES)
                )
        for offset in order:
            give_back(j, offset, c).start()
        rx2[j, ep * cores + c] = tx2[j, c, ep]
        if j == 0:

            @pl.when(is_late)
            def _():
                pl.semaphore_wait(pair_sem, 1)

            @pl.when(jnp.logical_and(c == 1, jnp.logical_not(is_root)))
            def _():
                pl.semaphore_wait(pair_sem, 1)
                pl.semaphore_wait(late_sem, 1)

        to_other_plane(j)

    total = shared_half[...]
    for j in range(chunks):
        arrived = rx2.at[j, pl.ds(0, experts * cores - 1)]
        pltpu.make_async_copy(arrived, arrived, recv2_sem.at[j]).wait()
        summed = dot(picks[j], rx2[j].reshape(experts * cores * thin, LANES))
        total = total + summed[: thin * local_tokens] + summed[thin * local_tokens :]
    squares = total * total
    mine = functools.reduce(jnp.add, [squares[q * local_tokens : (q + 1) * local_tokens] for q in range(thin)])
    mine = jnp.broadcast_to(jnp.sum(mine, axis=1, keepdims=True), (local_tokens, LANES))
    sq_send[...] = mine
    pair = pltpu.make_async_remote_copy(
        src_ref=sq_send, dst_ref=sq_recv, send_sem=pair_send.at[1], recv_sem=pair_recv.at[1],
        device_id={"tp": other}, device_id_type=MESH,
    )
    pair.start()
    for j in range(chunks):
        sent = tx.at[j, pl.ds(0, experts - 1)]
        pltpu.make_async_copy(sent, sent, send_sem.at[j]).wait()
        sent = rx2.at[j, pl.ds(0, experts * cores - 1)]
        pltpu.make_async_copy(sent, sent, send2_sem.at[j]).wait()
    @pl.when(is_mailbox)
    def _():
        for copy in forwards:
            copy.wait_send()

    pair.wait()
    scale = lax.rsqrt((mine + sq_recv[...]) / width + EPSILON)
    gains = out_gain[...].astype(F32)
    for q in range(thin):
        lanes = slice(q * LANES, (q + 1) * LANES)
        out_ref[:, lanes] = (total[q * local_tokens : (q + 1) * local_tokens] * scale * gains[q : q + 1, :]).astype(BF16)


def body(tokens, in_gain, route_expert, route_weight, gate_weight, up_weight, down_weight, shared_gate, shared_up, shared_down, out_gain):
    experts, cores = lax.axis_size("ep"), lax.axis_size("tp")
    local_tokens, width = tokens.shape
    top_count = route_expert.shape[1]
    slots = max(2, (local_tokens * top_count * 4 + 3 * experts - 1) // (3 * experts))
    chunks = slots // cores
    half = width // cores
    wide, thin = width // LANES, half // LANES
    hidden = gate_weight.shape[2]
    any_spec = pl.BlockSpec(memory_space=pl.ANY)
    vmem, dma = pltpu.VMEM, pltpu.SemaphoreType.DMA
    scratch = [
        vmem((local_tokens, width), BF16), vmem((wide, LANES), BF16), vmem((top_count, local_tokens), jnp.int32),
        vmem((top_count, local_tokens), F32), vmem((thin, LANES), BF16),
        vmem((cores, width, hidden), BF16), vmem((cores, width, hidden), BF16), vmem((cores, hidden, width), BF16),
        vmem((width, hidden), BF16), vmem((width, hidden), BF16), vmem((hidden, width), BF16),
        vmem((local_tokens, width), BF16),
        vmem((chunks, experts, wide, LANES), BF16), vmem((chunks, 2 * experts, wide, LANES), BF16),
        vmem((experts, width), BF16),
        vmem((chunks, cores, experts, thin, LANES), BF16), vmem((chunks, experts * cores, thin, LANES), BF16),
        vmem((chunks, 2 * thin * local_tokens, experts * cores * thin), BF16),
        vmem((cores, local_tokens, half), BF16), vmem((local_tokens, half), BF16), vmem((thin * local_tokens, LANES), F32),
        vmem((local_tokens, LANES), F32), vmem((local_tokens, LANES), F32),
        dma((5,)), dma((6,)), dma((3,)), dma((3,)), dma((chunks,)), dma((2 * chunks,)), dma((chunks,)), dma((chunks,)),
        dma((chunks,)), dma((2,)), dma((2,)), pltpu.SemaphoreType.REGULAR, pltpu.SemaphoreType.REGULAR,
    ]
    return pl.pallas_call(
        functools.partial(kernel, experts, cores, slots),
        out_shape=jax.ShapeDtypeStruct((local_tokens, half), BF16),
        in_specs=[any_spec] * 11,
        out_specs=pl.BlockSpec(memory_space=pltpu.VMEM),
        scratch_shapes=scratch,
        compiler_params=pltpu.CompilerParams(collective_id=0, has_side_effects=True, vmem_limit_bytes=60 * 1024 * 1024),
    )(
        tokens, in_gain.reshape(wide, LANES), route_expert.T, route_weight.T, gate_weight, up_weight, down_weight,
        shared_gate, shared_up, shared_down, out_gain.reshape(thin, LANES),
    )


def solution(mesh):
    return jax.shard_map(
        body,
        mesh=mesh,
        in_specs=(
            P(("grp", "ep"), None),
            P(),
            P(("grp", "ep"), None),
            P(("grp", "ep"), None),
            P("ep", None, "tp"),
            P("ep", None, "tp"),
            P("ep", "tp", None),
            P(None, "tp"),
            P(None, "tp"),
            P("tp", None),
            P("tp"),
        ),
        out_specs=P(("grp", "ep"), "tp"),
        check_vma=False,
    )
```

```python
import functools
import math

import jax
import jax.numpy as jnp
from jax import lax
from jax.experimental import pallas as pl
from jax.experimental.pallas import tpu as pltpu
from jax.sharding import PartitionSpec as P

EPSILON = 1e-06
BF16 = jnp.bfloat16
F32 = jnp.float32
LANES = 128
MESH = pl.DeviceIdType.MESH


def far_first(side):
    def reach(step):
        return min(step, side - step)

    offsets = [(dx, dy) for dy in range(side) for dx in range(side) if dx or dy]
    return sorted(offsets, key=lambda o: -(reach(o[0]) + reach(o[1])))


def dot(a, b):
    return jnp.dot(a, b, preferred_element_type=F32)


def iota(shape, dim):
    return lax.broadcasted_iota(jnp.int32, shape, dim)


def one_hot_to_rows(blocks, per_row):
    size = blocks * per_row
    row, col = iota((size, size), 0), iota((size, size), 1)
    return (col == (row % blocks) * per_row + row // blocks).astype(F32).astype(BF16)


def one_hot_to_blocks(blocks, per_row):
    size = blocks * per_row
    row, col = iota((size, size), 0), iota((size, size), 1)
    return (col == (row % per_row) * blocks + row // per_row).astype(F32).astype(BF16)


def kernel(
    experts, cores, slots,
    tokens_hbm, in_gain_hbm, route_hbm, weight_hbm, gate_hbm, up_hbm, down_hbm, sgate_hbm, sup_hbm, sdown_hbm, out_gain_hbm,
    out_ref,
    tokens, in_gain, route, weight, out_gain, gate, up, down, sgate, sup, sdown,
    normed, tx, rx, rows, tx2, rx2, picks, shared_send, shared_recv, shared_half, sq_send, sq_recv,
    small_sem, weight_sem, push_send, push_recv, send_sem, recv_sem, send2_sem, recv2_sem, forward_sem, pair_send, pair_recv, pair_sem, late_sem,
):
    ep, c = lax.axis_index("ep"), lax.axis_index("tp")
    other = 1 - c
    side = math.isqrt(experts)
    here_x, here_y = lax.rem(ep, side), lax.div(ep, side)
    local_tokens, width = tokens.shape
    half = width // cores
    chunks = slots // cores
    wide = width // LANES
    thin = half // LANES
    order = far_first(side)
    is_root = ep == 0
    is_late = jnp.logical_and(is_root, c == 0)
    is_mailbox = jnp.logical_and(is_root, c == 1)
    counts_partner = is_root == (c == 0)

    def peer(offset):
        return lax.rem(here_y + offset[1], side) * side + lax.rem(here_x + offset[0], side)

    small = [
        pltpu.make_async_copy(src, dst, small_sem.at[i])
        for i, (src, dst) in enumerate(
            [(route_hbm, route), (tokens_hbm, tokens), (in_gain_hbm, in_gain), (weight_hbm, weight), (out_gain_hbm, out_gain)]
        )
    ]
    for copy in small:
        copy.start()
    barrier = pltpu.get_barrier_semaphore()

    @pl.when(jnp.logical_not(is_late))
    def _():
        for offset in order:
            pl.semaphore_signal(barrier, inc=1, device_id={"ep": peer(offset)}, device_id_type=MESH)

    @pl.when(jnp.logical_not(counts_partner))
    def _():
        pl.semaphore_signal(barrier, inc=1, device_id={"tp": other}, device_id_type=MESH)

    pushes = [
        pltpu.make_async_remote_copy(
            src_ref=src.at[0], dst_ref=dst.at[1], send_sem=push_send.at[i], recv_sem=push_recv.at[i],
            device_id={"tp": other}, device_id_type=MESH,
        )
        for i, (src, dst) in enumerate([(gate_hbm, gate), (up_hbm, up), (down_hbm, down)])
    ]

    def tell_partner():
        pl.semaphore_signal(pair_sem, inc=1, device_id={"tp": other}, device_id_type=MESH)

    def push():
        for copy in pushes:
            copy.start()

    @pl.when(jnp.logical_and(c == 0, is_root))
    def _():
        pl.semaphore_wait(barrier, experts)
        tell_partner()
        push()

    loads = [
        pltpu.make_async_copy(src, dst, weight_sem.at[i])
        for i, (src, dst) in enumerate(
            [
                (sgate_hbm, sgate), (sup_hbm, sup), (sdown_hbm, sdown),
                (gate_hbm.at[0], gate.at[0]), (up_hbm.at[0], up.at[0]), (down_hbm.at[0], down.at[0]),
            ]
        )
    ]
    for copy in loads:
        copy.start()

    small[0].wait()
    names = route[...]
    expert_row = iota((experts, local_tokens), 0)
    hits = [names[k : k + 1, :] == expert_row for k in range(names.shape[0])]
    chosen = functools.reduce(jnp.logical_or, hits)
    earlier = (iota((local_tokens, local_tokens), 0) < iota((local_tokens, local_tokens), 1)).astype(F32).astype(BF16)
    rank_t = jnp.where(chosen, dot(chosen.astype(F32).astype(BF16), earlier), -1.0)

    small[1].wait()
    small[2].wait()
    floats = tokens[...].astype(F32)
    scale = lax.rsqrt(jnp.mean(floats * floats, axis=1, keepdims=True) + EPSILON)
    gains = in_gain[...].astype(F32)
    for q in range(wide):
        lanes = slice(q * LANES, (q + 1) * LANES)
        normed[:, lanes] = (floats[:, lanes] * scale * gains[q : q + 1, :]).astype(BF16)

    to_blocks = one_hot_to_blocks(wide, wide)
    per_block = wide
    first_slot = (c * chunks).astype(F32)
    for j in range(chunks):
        pick = (rank_t == first_slot + j).astype(F32).astype(BF16)
        picked = dot(pick, normed[...]).astype(BF16)
        for b in range(experts // per_block):
            part = picked[b * per_block : (b + 1) * per_block]
            stacked = jnp.concatenate([part[:, q * LANES : (q + 1) * LANES] for q in range(wide)], axis=0)
            tx[j, pl.ds(b * per_block, per_block)] = (
                dot(to_blocks, stacked).astype(BF16).reshape(per_block, wide, LANES)
            )
        rx[j, ep] = tx[j, ep]

    def dispatch(j, to):
        redirect = jnp.logical_and(to == 0, c == 0).astype(jnp.int32)
        return pltpu.make_async_remote_copy(
            src_ref=tx.at[j, to], dst_ref=rx.at[j, ep + redirect * experts], send_sem=send_sem.at[j],
            recv_sem=recv_sem.at[j + redirect * chunks], device_id={"ep": to, "tp": c + redirect}, device_id_type=MESH,
        )

    forwards = [
        pltpu.make_async_remote_copy(
            src_ref=rx.at[j, pl.ds(experts + 1, experts - 1)], dst_ref=rx.at[j, pl.ds(1, experts - 1)],
            send_sem=forward_sem.at[j], recv_sem=recv_sem.at[j], device_id={"tp": 0}, device_id_type=MESH,
        )
        for j in range(chunks)
    ]

    @pl.when(jnp.logical_and(c == 0, jnp.logical_not(is_root)))
    def _():
        pl.semaphore_wait(pair_sem, 1)
        pl.semaphore_wait(barrier, experts - 2)
        tell_partner()

    @pl.when(jnp.logical_and(c == 1, is_root))
    def _():
        pl.semaphore_wait(barrier, experts - 1)

    @pl.when(jnp.logical_and(c == 1, jnp.logical_not(is_root)))
    def _():
        pl.semaphore_wait(barrier, experts)
        tell_partner()

    for j in range(chunks):
        for offset in order:
            dispatch(j, peer(offset)).start()
        if j == 0:

            @pl.when(is_late)
            def _():
                for offset in order:
                    pl.semaphore_signal(late_sem, inc=1, device_id={"ep": peer(offset)}, device_id_type=MESH)

    @pl.when(jnp.logical_and(c == 1, is_root))
    def _():
        pl.semaphore_wait(pair_sem, 1)
        tell_partner()

    @pl.when(jnp.logical_not(is_late))
    def _():
        push()

    def swiglu(inputs, pairs):
        hidden = []
        for gate_here, up_here in pairs:
            gate_value = dot(inputs, gate_here)
            upward = dot(inputs, up_here)
            hidden.append((jax.nn.silu(gate_value) * upward).astype(BF16))
        return hidden

    for copy in loads[:3]:
        copy.wait()
    (hidden,) = swiglu(normed[...], [(sgate[...], sup[...])])
    shared_part = dot(hidden, sdown[...]).astype(BF16)
    for side_of in range(cores):
        shared_send[side_of] = shared_part[:, side_of * half : (side_of + 1) * half]
    pair = pltpu.make_async_remote_copy(
        src_ref=shared_send.at[other], dst_ref=shared_recv, send_sem=pair_send.at[0], recv_sem=pair_recv.at[0],
        device_id={"tp": other}, device_id_type=MESH,
    )
    pair.start()

    small[3].wait()
    small[4].wait()
    weights = weight[...]
    weight_t = functools.reduce(jnp.add, [jnp.where(hit, weights[k : k + 1, :], 0.0) for k, hit in enumerate(hits)])
    high = weight_t.astype(BF16)
    low = (weight_t - high.astype(F32)).astype(BF16)
    eye = (iota((local_tokens, local_tokens), 0) == iota((local_tokens, local_tokens), 1)).astype(F32).astype(BF16)
    turned = [
        lax.dot_general(eye, part, (((1,), (1,)), ((), ())), preferred_element_type=F32).astype(BF16)
        for part in (high, low, rank_t.astype(BF16))
    ]
    columns = experts * cores * thin
    expand = (iota((experts, columns), 0) == iota((experts, columns), 1) // (cores * thin)).astype(F32).astype(BF16)
    spread = dot(jnp.concatenate(turned, axis=0), expand)
    col = iota((local_tokens, columns), 1)
    slot_base = ((col // thin) % cores * chunks).astype(F32)
    q_col = col % thin
    for j in range(chunks):
        here = spread[2 * local_tokens :] == slot_base + j
        for part in range(2):
            value = jnp.where(here, spread[part * local_tokens : (part + 1) * local_tokens], 0.0)
            for q in range(thin):
                picks[j, pl.ds((part * thin + q) * local_tokens, local_tokens)] = jnp.where(
                    q_col == q, value, 0.0
                ).astype(BF16)

    pair.wait()
    for q in range(thin):
        lanes = slice(q * LANES, (q + 1) * LANES)
        total = shared_send[c][:, lanes].astype(F32) + shared_recv[:, lanes].astype(F32)
        shared_half[pl.ds(q * local_tokens, local_tokens)] = total.astype(BF16).astype(F32)

    @pl.when(jnp.logical_and(c == 0, jnp.logical_not(is_root)))
    def _():
        pl.semaphore_wait(late_sem, 1)
        pl.semaphore_signal(late_sem, inc=1, device_id={"tp": 1}, device_id_type=MESH)

    def forward(j):
        @pl.when(is_mailbox)
        def _():
            arrived = rx.at[j, pl.ds(experts + 1, experts - 1)]
            pltpu.make_async_copy(arrived, arrived, recv_sem.at[chunks + j]).wait()
            forwards[j].start()

    forward(0)
    for copy in loads[3:]:
        copy.wait()
    for copy in pushes:
        copy.wait()

    to_rows = one_hot_to_rows(wide, wide)
    per_back = 2 * LANES // thin
    to_thin = one_hot_to_blocks(per_back, thin)

    def give_back(j, offset, core):
        to = peer(offset)
        return pltpu.make_async_remote_copy(
            src_ref=tx2.at[j, core, to], dst_ref=rx2.at[j, ep * cores + c], send_sem=send2_sem.at[j], recv_sem=recv2_sem.at[j],
            device_id={"ep": to, "tp": core}, device_id_type=MESH,
        )

    def to_other_plane(j):
        for offset in order:
            give_back(j, offset, other).start()
        back = pltpu.make_async_remote_copy(
            src_ref=tx2.at[j, other, ep], dst_ref=rx2.at[j, ep * cores + c], send_sem=send2_sem.at[j], recv_sem=recv2_sem.at[j],
            device_id={"tp": other}, device_id_type=MESH,
        )
        back.start()

    for j in range(chunks):
        if j:
            forward(j)
        arrived = rx.at[j, pl.ds(0, experts - 1)]
        pltpu.make_async_copy(arrived, arrived, recv_sem.at[j]).wait()
        for b in range(experts // per_block):
            block = rx[j, pl.ds(b * per_block, per_block)].reshape(per_block * wide, LANES)
            sorted_rows = dot(to_rows, block).astype(BF16)
            for q in range(wide):
                rows[pl.ds(b * per_block, per_block), q * LANES : (q + 1) * LANES] = sorted_rows[
                    q * per_block : (q + 1) * per_block
                ]
        hidden = swiglu(rows[...], [(gate[h], up[h]) for h in range(cores)])
        result = functools.reduce(jnp.add, [dot(hidden[h], down[h]) for h in range(cores)]).astype(BF16)
        for b in range(experts // per_back):
            part = result[b * per_back : (b + 1) * per_back]
            for core in range(cores):
                stacked = jnp.concatenate(
                    [part[:, core * half + q * LANES : core * half + (q + 1) * LANES] for q in range(thin)], axis=0
                )
                tx2[j, core, pl.ds(b * per_back, per_back)] = (
                    dot(to_thin, stacked).astype(BF16).reshape(per_back, thin, LANES)
                )
        for offset in order:
            give_back(j, offset, c).start()
        rx2[j, ep * cores + c] = tx2[j, c, ep]
        if j == 0:

            @pl.when(is_late)
            def _():
                pl.semaphore_wait(pair_sem, 1)

            @pl.when(jnp.logical_and(c == 1, jnp.logical_not(is_root)))
            def _():
                pl.semaphore_wait(pair_sem, 1)
                pl.semaphore_wait(late_sem, 1)

        to_other_plane(j)

    total = shared_half[...]
    for j in range(chunks):
        arrived = rx2.at[j, pl.ds(0, experts * cores - 1)]
        pltpu.make_async_copy(arrived, arrived, recv2_sem.at[j]).wait()
        summed = dot(picks[j], rx2[j].reshape(experts * cores * thin, LANES))
        total = total + summed[: thin * local_tokens] + summed[thin * local_tokens :]
    squares = total * total
    mine = functools.reduce(jnp.add, [squares[q * local_tokens : (q + 1) * local_tokens] for q in range(thin)])
    mine = jnp.broadcast_to(jnp.sum(mine, axis=1, keepdims=True), (local_tokens, LANES))
    sq_send[...] = mine
    pair = pltpu.make_async_remote_copy(
        src_ref=sq_send, dst_ref=sq_recv, send_sem=pair_send.at[1], recv_sem=pair_recv.at[1],
        device_id={"tp": other}, device_id_type=MESH,
    )
    pair.start()
    for j in range(chunks):
        sent = tx.at[j, pl.ds(0, experts - 1)]
        pltpu.make_async_copy(sent, sent, send_sem.at[j]).wait()
        sent = rx2.at[j, pl.ds(0, experts * cores - 1)]
        pltpu.make_async_copy(sent, sent, send2_sem.at[j]).wait()
    @pl.when(is_mailbox)
    def _():
        for copy in forwards:
            copy.wait_send()

    pair.wait()
    scale = lax.rsqrt((mine + sq_recv[...]) / width + EPSILON)
    gains = out_gain[...].astype(F32)
    for q in range(thin):
        lanes = slice(q * LANES, (q + 1) * LANES)
        out_ref[:, lanes] = (total[q * local_tokens : (q + 1) * local_tokens] * scale * gains[q : q + 1, :]).astype(BF16)


def body(tokens, in_gain, route_expert, route_weight, gate_weight, up_weight, down_weight, shared_gate, shared_up, shared_down, out_gain):
    experts, cores = lax.axis_size("ep"), lax.axis_size("tp")
    local_tokens, width = tokens.shape
    top_count = route_expert.shape[1]
    slots = max(2, (local_tokens * top_count * 4 + 3 * experts - 1) // (3 * experts))
    chunks = slots // cores
    half = width // cores
    wide, thin = width // LANES, half // LANES
    hidden = gate_weight.shape[2]
    any_spec = pl.BlockSpec(memory_space=pl.ANY)
    vmem, dma = pltpu.VMEM, pltpu.SemaphoreType.DMA
    scratch = [
        vmem((local_tokens, width), BF16), vmem((wide, LANES), BF16), vmem((top_count, local_tokens), jnp.int32),
        vmem((top_count, local_tokens), F32), vmem((thin, LANES), BF16),
        vmem((cores, width, hidden), BF16), vmem((cores, width, hidden), BF16), vmem((cores, hidden, width), BF16),
        vmem((width, hidden), BF16), vmem((width, hidden), BF16), vmem((hidden, width), BF16),
        vmem((local_tokens, width), BF16),
        vmem((chunks, experts, wide, LANES), BF16), vmem((chunks, 2 * experts, wide, LANES), BF16),
        vmem((experts, width), BF16),
        vmem((chunks, cores, experts, thin, LANES), BF16), vmem((chunks, experts * cores, thin, LANES), BF16),
        vmem((chunks, 2 * thin * local_tokens, experts * cores * thin), BF16),
        vmem((cores, local_tokens, half), BF16), vmem((local_tokens, half), BF16), vmem((thin * local_tokens, LANES), F32),
        vmem((local_tokens, LANES), F32), vmem((local_tokens, LANES), F32),
        dma((5,)), dma((6,)), dma((3,)), dma((3,)), dma((chunks,)), dma((2 * chunks,)), dma((chunks,)), dma((chunks,)),
        dma((chunks,)), dma((2,)), dma((2,)), pltpu.SemaphoreType.REGULAR, pltpu.SemaphoreType.REGULAR,
    ]
    return pl.pallas_call(
        functools.partial(kernel, experts, cores, slots),
        out_shape=jax.ShapeDtypeStruct((local_tokens, half), BF16),
        in_specs=[any_spec] * 11,
        out_specs=pl.BlockSpec(memory_space=pltpu.VMEM),
        scratch_shapes=scratch,
        compiler_params=pltpu.CompilerParams(collective_id=0, has_side_effects=True, vmem_limit_bytes=60 * 1024 * 1024),
    )(
        tokens, in_gain.reshape(wide, LANES), route_expert.T, route_weight.T, gate_weight, up_weight, down_weight,
        shared_gate, shared_up, shared_down, out_gain.reshape(thin, LANES),
    )


def solution(mesh):
    return jax.shard_map(
        body,
        mesh=mesh,
        in_specs=(
            P(("grp", "ep"), None),
            P(),
            P(("grp", "ep"), None),
            P(("grp", "ep"), None),
            P("ep", None, "tp"),
            P("ep", None, "tp"),
            P("ep", "tp", None),
            P(None, "tp"),
            P(None, "tp"),
            P("tp", None),
            P("tp"),
        ),
        out_specs=P(("grp", "ep"), "tp"),
        check_vma=False,
    )
```

```python
import functools
import math

import jax
import jax.numpy as jnp
from jax import lax
from jax.experimental import pallas as pl
from jax.experimental.pallas import tpu as pltpu
from jax.sharding import PartitionSpec as P

EPSILON = 1e-06
BF16 = jnp.bfloat16
F32 = jnp.float32
LANES = 128
MESH = pl.DeviceIdType.MESH


def far_first(side):
    def reach(step):
        return min(step, side - step)

    offsets = [(dx, dy) for dy in range(side) for dx in range(side) if dx or dy]
    return sorted(offsets, key=lambda o: -(reach(o[0]) + reach(o[1])))


def dot(a, b):
    return jnp.dot(a, b, preferred_element_type=F32)


def iota(shape, dim):
    return lax.broadcasted_iota(jnp.int32, shape, dim)


def one_hot_to_rows(blocks, per_row):
    size = blocks * per_row
    row, col = iota((size, size), 0), iota((size, size), 1)
    return (col == (row % blocks) * per_row + row // blocks).astype(F32).astype(BF16)


def one_hot_to_blocks(blocks, per_row):
    size = blocks * per_row
    row, col = iota((size, size), 0), iota((size, size), 1)
    return (col == (row % per_row) * blocks + row // per_row).astype(F32).astype(BF16)


def kernel(
    experts, cores, slots,
    tokens_hbm, in_gain_hbm, route_hbm, weight_hbm, gate_hbm, up_hbm, down_hbm, sgate_hbm, sup_hbm, sdown_hbm, out_gain_hbm,
    out_ref,
    tokens, in_gain, route, weight, out_gain, gate, up, down, sgate, sup, sdown,
    normed, tx, rx, rows, tx2, rx2, picks, shared_send, shared_recv, shared_half, sq_send, sq_recv,
    small_sem, weight_sem, push_send, push_recv, send_sem, recv_sem, send2_sem, recv2_sem, forward_sem, pair_send, pair_recv, pair_sem, late_sem,
):
    ep, c = lax.axis_index("ep"), lax.axis_index("tp")
    other = 1 - c
    side = math.isqrt(experts)
    here_x, here_y = lax.rem(ep, side), lax.div(ep, side)
    local_tokens, width = tokens.shape
    half = width // cores
    chunks = slots // cores
    wide = width // LANES
    thin = half // LANES
    order = far_first(side)
    is_root = ep == 0
    is_late = jnp.logical_and(is_root, c == 0)
    is_mailbox = jnp.logical_and(is_root, c == 1)
    counts_partner = is_root == (c == 0)

    def peer(offset):
        return lax.rem(here_y + offset[1], side) * side + lax.rem(here_x + offset[0], side)

    small = [
        pltpu.make_async_copy(src, dst, small_sem.at[i])
        for i, (src, dst) in enumerate(
            [(route_hbm, route), (tokens_hbm, tokens), (in_gain_hbm, in_gain), (weight_hbm, weight), (out_gain_hbm, out_gain)]
        )
    ]
    for copy in small:
        copy.start()
    barrier = pltpu.get_barrier_semaphore()

    @pl.when(jnp.logical_not(is_late))
    def _():
        for offset in order:
            pl.semaphore_signal(barrier, inc=1, device_id={"ep": peer(offset)}, device_id_type=MESH)

    @pl.when(jnp.logical_not(counts_partner))
    def _():
        pl.semaphore_signal(barrier, inc=1, device_id={"tp": other}, device_id_type=MESH)

    pushes = [
        pltpu.make_async_remote_copy(
            src_ref=src.at[0], dst_ref=dst.at[1], send_sem=push_send.at[i], recv_sem=push_recv.at[i],
            device_id={"tp": other}, device_id_type=MESH,
        )
        for i, (src, dst) in enumerate([(gate_hbm, gate), (up_hbm, up), (down_hbm, down)])
    ]

    def tell_partner():
        pl.semaphore_signal(pair_sem, inc=1, device_id={"tp": other}, device_id_type=MESH)

    def push():
        for copy in pushes:
            copy.start()

    @pl.when(jnp.logical_and(c == 0, is_root))
    def _():
        pl.semaphore_wait(barrier, experts)
        tell_partner()
        push()

    loads = [
        pltpu.make_async_copy(src, dst, weight_sem.at[i])
        for i, (src, dst) in enumerate(
            [
                (sgate_hbm, sgate), (sup_hbm, sup), (sdown_hbm, sdown),
                (gate_hbm.at[0], gate.at[0]), (up_hbm.at[0], up.at[0]), (down_hbm.at[0], down.at[0]),
            ]
        )
    ]
    for copy in loads:
        copy.start()

    small[0].wait()
    names = route[...]
    expert_row = iota((experts, local_tokens), 0)
    hits = [names[k : k + 1, :] == expert_row for k in range(names.shape[0])]
    chosen = functools.reduce(jnp.logical_or, hits)
    earlier = (iota((local_tokens, local_tokens), 0) < iota((local_tokens, local_tokens), 1)).astype(F32).astype(BF16)
    rank_t = jnp.where(chosen, dot(chosen.astype(F32).astype(BF16), earlier), -1.0)

    small[1].wait()
    small[2].wait()
    floats = tokens[...].astype(F32)
    scale = lax.rsqrt(jnp.mean(floats * floats, axis=1, keepdims=True) + EPSILON)
    gains = in_gain[...].astype(F32)
    for q in range(wide):
        lanes = slice(q * LANES, (q + 1) * LANES)
        normed[:, lanes] = (floats[:, lanes] * scale * gains[q : q + 1, :]).astype(BF16)

    to_blocks = one_hot_to_blocks(wide, wide)
    per_block = wide
    first_slot = (c * chunks).astype(F32)
    for j in range(chunks):
        pick = (rank_t == first_slot + j).astype(F32).astype(BF16)
        picked = dot(pick, normed[...]).astype(BF16)
        for b in range(experts // per_block):
            part = picked[b * per_block : (b + 1) * per_block]
            stacked = jnp.concatenate([part[:, q * LANES : (q + 1) * LANES] for q in range(wide)], axis=0)
            tx[j, pl.ds(b * per_block, per_block)] = (
                dot(to_blocks, stacked).astype(BF16).reshape(per_block, wide, LANES)
            )
        rx[j, ep] = tx[j, ep]

    def dispatch(j, to):
        redirect = jnp.logical_and(to == 0, c == 0).astype(jnp.int32)
        return pltpu.make_async_remote_copy(
            src_ref=tx.at[j, to], dst_ref=rx.at[j, ep + redirect * experts], send_sem=send_sem.at[j],
            recv_sem=recv_sem.at[j + redirect * chunks], device_id={"ep": to, "tp": c + redirect}, device_id_type=MESH,
        )

    forwards = [
        pltpu.make_async_remote_copy(
            src_ref=rx.at[j, pl.ds(experts + 1, experts - 1)], dst_ref=rx.at[j, pl.ds(1, experts - 1)],
            send_sem=forward_sem.at[j], recv_sem=recv_sem.at[j], device_id={"tp": 0}, device_id_type=MESH,
        )
        for j in range(chunks)
    ]

    @pl.when(jnp.logical_and(c == 0, jnp.logical_not(is_root)))
    def _():
        pl.semaphore_wait(pair_sem, 1)
        pl.semaphore_wait(barrier, experts - 2)
        tell_partner()

    @pl.when(jnp.logical_and(c == 1, is_root))
    def _():
        pl.semaphore_wait(barrier, experts - 1)

    @pl.when(jnp.logical_and(c == 1, jnp.logical_not(is_root)))
    def _():
        pl.semaphore_wait(barrier, experts)
        tell_partner()

    for j in range(chunks):
        for offset in order:
            dispatch(j, peer(offset)).start()
        if j == 0:

            @pl.when(is_late)
            def _():
                for offset in order:
                    pl.semaphore_signal(late_sem, inc=1, device_id={"ep": peer(offset)}, device_id_type=MESH)

    @pl.when(jnp.logical_and(c == 1, is_root))
    def _():
        pl.semaphore_wait(pair_sem, 1)
        tell_partner()

    @pl.when(jnp.logical_not(is_late))
    def _():
        push()

    def swiglu(inputs, pairs):
        hidden = []
        for gate_here, up_here in pairs:
            gate_value = dot(inputs, gate_here)
            upward = dot(inputs, up_here)
            hidden.append((jax.nn.silu(gate_value) * upward).astype(BF16))
        return hidden

    for copy in loads[:3]:
        copy.wait()
    (hidden,) = swiglu(normed[...], [(sgate[...], sup[...])])
    shared_part = dot(hidden, sdown[...]).astype(BF16)
    for side_of in range(cores):
        shared_send[side_of] = shared_part[:, side_of * half : (side_of + 1) * half]
    pair = pltpu.make_async_remote_copy(
        src_ref=shared_send.at[other], dst_ref=shared_recv, send_sem=pair_send.at[0], recv_sem=pair_recv.at[0],
        device_id={"tp": other}, device_id_type=MESH,
    )
    pair.start()

    small[3].wait()
    small[4].wait()
    weights = weight[...]
    weight_t = functools.reduce(jnp.add, [jnp.where(hit, weights[k : k + 1, :], 0.0) for k, hit in enumerate(hits)])
    high = weight_t.astype(BF16)
    low = (weight_t - high.astype(F32)).astype(BF16)
    eye = (iota((local_tokens, local_tokens), 0) == iota((local_tokens, local_tokens), 1)).astype(F32).astype(BF16)
    turned = [
        lax.dot_general(eye, part, (((1,), (1,)), ((), ())), preferred_element_type=F32).astype(BF16)
        for part in (high, low, rank_t.astype(BF16))
    ]
    columns = experts * cores * thin
    expand = (iota((experts, columns), 0) == iota((experts, columns), 1) // (cores * thin)).astype(F32).astype(BF16)
    spread = dot(jnp.concatenate(turned, axis=0), expand)
    col = iota((local_tokens, columns), 1)
    slot_base = ((col // thin) % cores * chunks).astype(F32)
    q_col = col % thin
    for j in range(chunks):
        here = spread[2 * local_tokens :] == slot_base + j
        for part in range(2):
            value = jnp.where(here, spread[part * local_tokens : (part + 1) * local_tokens], 0.0)
            for q in range(thin):
                picks[j, pl.ds((part * thin + q) * local_tokens, local_tokens)] = jnp.where(
                    q_col == q, value, 0.0
                ).astype(BF16)

    def forward(j):
        @pl.when(is_mailbox)
        def _():
            arrived = rx.at[j, pl.ds(experts + 1, experts - 1)]
            pltpu.make_async_copy(arrived, arrived, recv_sem.at[chunks + j]).wait()
            forwards[j].start()

    forward(0)
    pair.wait()
    for q in range(thin):
        lanes = slice(q * LANES, (q + 1) * LANES)
        total = shared_send[c][:, lanes].astype(F32) + shared_recv[:, lanes].astype(F32)
        shared_half[pl.ds(q * local_tokens, local_tokens)] = total.astype(BF16).astype(F32)

    @pl.when(jnp.logical_and(c == 0, jnp.logical_not(is_root)))
    def _():
        pl.semaphore_wait(late_sem, 1)
        pl.semaphore_signal(late_sem, inc=1, device_id={"tp": 1}, device_id_type=MESH)

    for copy in loads[3:]:
        copy.wait()
    for copy in pushes[:2]:
        copy.wait()

    to_rows = one_hot_to_rows(wide, wide)
    per_back = 2 * LANES // thin
    to_thin = one_hot_to_blocks(per_back, thin)

    def give_back(j, offset, core):
        to = peer(offset)
        return pltpu.make_async_remote_copy(
            src_ref=tx2.at[j, core, to], dst_ref=rx2.at[j, ep * cores + c], send_sem=send2_sem.at[j], recv_sem=recv2_sem.at[j],
            device_id={"ep": to, "tp": core}, device_id_type=MESH,
        )

    def to_partner(j):
        pltpu.make_async_remote_copy(
            src_ref=tx2.at[j, other, ep], dst_ref=rx2.at[j, ep * cores + c], send_sem=send2_sem.at[j], recv_sem=recv2_sem.at[j],
            device_id={"tp": other}, device_id_type=MESH,
        ).start()

    for j in range(chunks):
        arrived = rx.at[j, pl.ds(0, experts - 1)]
        pltpu.make_async_copy(arrived, arrived, recv_sem.at[j]).wait()
        for b in range(experts // per_block):
            block = rx[j, pl.ds(b * per_block, per_block)].reshape(per_block * wide, LANES)
            sorted_rows = dot(to_rows, block).astype(BF16)
            for q in range(wide):
                rows[pl.ds(b * per_block, per_block), q * LANES : (q + 1) * LANES] = sorted_rows[
                    q * per_block : (q + 1) * per_block
                ]
        hidden = swiglu(rows[...], [(gate[h], up[h]) for h in range(cores)])
        if j == 0:
            pushes[2].wait()
        result = functools.reduce(jnp.add, [dot(hidden[h], down[h]) for h in range(cores)]).astype(BF16)
        for b in range(experts // per_back):
            part = result[b * per_back : (b + 1) * per_back]
            for core in range(cores):
                stacked = jnp.concatenate(
                    [part[:, core * half + q * LANES : core * half + (q + 1) * LANES] for q in range(thin)], axis=0
                )
                tx2[j, core, pl.ds(b * per_back, per_back)] = (
                    dot(to_thin, stacked).astype(BF16).reshape(per_back, thin, LANES)
                )
        rx2[j, ep * cores + c] = tx2[j, c, ep]
        if j + 1 < chunks:
            forward(j + 1)
        if j == 0:
            for offset in order:
                give_back(j, offset, c).start()

            @pl.when(is_late)
            def _():
                pl.semaphore_wait(pair_sem, 1)

            @pl.when(jnp.logical_and(c == 1, jnp.logical_not(is_root)))
            def _():
                pl.semaphore_wait(pair_sem, 1)
                pl.semaphore_wait(late_sem, 1)

            for offset in order:
                give_back(j, offset, other).start()
        else:
            for offset in order:
                give_back(j, offset, c).start()
                give_back(j, offset, other).start()
        to_partner(j)

    total = shared_half[...]
    for j in range(chunks):
        arrived = rx2.at[j, pl.ds(0, experts * cores - 1)]
        pltpu.make_async_copy(arrived, arrived, recv2_sem.at[j]).wait()
        summed = dot(picks[j], rx2[j].reshape(experts * cores * thin, LANES))
        total = total + summed[: thin * local_tokens] + summed[thin * local_tokens :]
    squares = total * total
    mine = functools.reduce(jnp.add, [squares[q * local_tokens : (q + 1) * local_tokens] for q in range(thin)])
    mine = jnp.broadcast_to(jnp.sum(mine, axis=1, keepdims=True), (local_tokens, LANES))
    sq_send[...] = mine
    pair = pltpu.make_async_remote_copy(
        src_ref=sq_send, dst_ref=sq_recv, send_sem=pair_send.at[1], recv_sem=pair_recv.at[1],
        device_id={"tp": other}, device_id_type=MESH,
    )
    pair.start()
    for j in range(chunks):
        sent = tx.at[j, pl.ds(0, experts - 1)]
        pltpu.make_async_copy(sent, sent, send_sem.at[j]).wait()
        sent = rx2.at[j, pl.ds(0, experts * cores - 1)]
        pltpu.make_async_copy(sent, sent, send2_sem.at[j]).wait()
    @pl.when(is_mailbox)
    def _():
        for copy in forwards:
            copy.wait_send()

    pair.wait()
    scale = lax.rsqrt((mine + sq_recv[...]) / width + EPSILON)
    gains = out_gain[...].astype(F32)
    for q in range(thin):
        lanes = slice(q * LANES, (q + 1) * LANES)
        out_ref[:, lanes] = (total[q * local_tokens : (q + 1) * local_tokens] * scale * gains[q : q + 1, :]).astype(BF16)


def body(tokens, in_gain, route_expert, route_weight, gate_weight, up_weight, down_weight, shared_gate, shared_up, shared_down, out_gain):
    experts, cores = lax.axis_size("ep"), lax.axis_size("tp")
    local_tokens, width = tokens.shape
    top_count = route_expert.shape[1]
    slots = max(2, (local_tokens * top_count * 4 + 3 * experts - 1) // (3 * experts))
    chunks = slots // cores
    half = width // cores
    wide, thin = width // LANES, half // LANES
    hidden = gate_weight.shape[2]
    any_spec = pl.BlockSpec(memory_space=pl.ANY)
    vmem, dma = pltpu.VMEM, pltpu.SemaphoreType.DMA
    scratch = [
        vmem((local_tokens, width), BF16), vmem((wide, LANES), BF16), vmem((top_count, local_tokens), jnp.int32),
        vmem((top_count, local_tokens), F32), vmem((thin, LANES), BF16),
        vmem((cores, width, hidden), BF16), vmem((cores, width, hidden), BF16), vmem((cores, hidden, width), BF16),
        vmem((width, hidden), BF16), vmem((width, hidden), BF16), vmem((hidden, width), BF16),
        vmem((local_tokens, width), BF16),
        vmem((chunks, experts, wide, LANES), BF16), vmem((chunks, 2 * experts, wide, LANES), BF16),
        vmem((experts, width), BF16),
        vmem((chunks, cores, experts, thin, LANES), BF16), vmem((chunks, experts * cores, thin, LANES), BF16),
        vmem((chunks, 2 * thin * local_tokens, experts * cores * thin), BF16),
        vmem((cores, local_tokens, half), BF16), vmem((local_tokens, half), BF16), vmem((thin * local_tokens, LANES), F32),
        vmem((local_tokens, LANES), F32), vmem((local_tokens, LANES), F32),
        dma((5,)), dma((6,)), dma((3,)), dma((3,)), dma((chunks,)), dma((2 * chunks,)), dma((chunks,)), dma((chunks,)),
        dma((chunks,)), dma((2,)), dma((2,)), pltpu.SemaphoreType.REGULAR, pltpu.SemaphoreType.REGULAR,
    ]
    return pl.pallas_call(
        functools.partial(kernel, experts, cores, slots),
        out_shape=jax.ShapeDtypeStruct((local_tokens, half), BF16),
        in_specs=[any_spec] * 11,
        out_specs=pl.BlockSpec(memory_space=pltpu.VMEM),
        scratch_shapes=scratch,
        compiler_params=pltpu.CompilerParams(collective_id=0, has_side_effects=True, vmem_limit_bytes=60 * 1024 * 1024),
    )(
        tokens, in_gain.reshape(wide, LANES), route_expert.T, route_weight.T, gate_weight, up_weight, down_weight,
        shared_gate, shared_up, shared_down, out_gain.reshape(thin, LANES),
    )


def solution(mesh):
    return jax.shard_map(
        body,
        mesh=mesh,
        in_specs=(
            P(("grp", "ep"), None),
            P(),
            P(("grp", "ep"), None),
            P(("grp", "ep"), None),
            P("ep", None, "tp"),
            P("ep", None, "tp"),
            P("ep", "tp", None),
            P(None, "tp"),
            P(None, "tp"),
            P("tp", None),
            P("tp"),
        ),
        out_specs=P(("grp", "ep"), "tp"),
        check_vma=False,
    )
```

```python
import functools
import math

import jax
import jax.numpy as jnp
from jax import lax
from jax.experimental import pallas as pl
from jax.experimental.pallas import tpu as pltpu
from jax.sharding import PartitionSpec as P

EPSILON = 1e-06
BF16 = jnp.bfloat16
F32 = jnp.float32
LANES = 128
MESH = pl.DeviceIdType.MESH


def far_first(side):
    def reach(step):
        return min(step, side - step)

    offsets = [(dx, dy) for dy in range(side) for dx in range(side) if dx or dy]
    return sorted(offsets, key=lambda o: -(reach(o[0]) + reach(o[1])))


def dot(a, b):
    return jnp.dot(a, b, preferred_element_type=F32)


def iota(shape, dim):
    return lax.broadcasted_iota(jnp.int32, shape, dim)


def one_hot_to_rows(blocks, per_row):
    size = blocks * per_row
    row, col = iota((size, size), 0), iota((size, size), 1)
    return (col == (row % blocks) * per_row + row // blocks).astype(F32).astype(BF16)


def one_hot_to_blocks(blocks, per_row):
    size = blocks * per_row
    row, col = iota((size, size), 0), iota((size, size), 1)
    return (col == (row % per_row) * blocks + row // per_row).astype(F32).astype(BF16)


def kernel(
    experts, cores, slots,
    tokens_hbm, in_gain_hbm, route_hbm, weight_hbm, gate_hbm, up_hbm, down_hbm, sgate_hbm, sup_hbm, sdown_hbm, out_gain_hbm,
    out_ref,
    tokens, in_gain, route, weight, out_gain, gate, up, down, sgate, sup, sdown,
    normed, tx, rx, rows, tx2, rx2, picks, shared_send, shared_recv, shared_half, sq_send, sq_recv,
    small_sem, weight_sem, push_send, push_recv, send_sem, recv_sem, send2_sem, recv2_sem, forward_sem, pair_send, pair_recv, pair_sem, late_sem,
):
    ep, c = lax.axis_index("ep"), lax.axis_index("tp")
    other = 1 - c
    side = math.isqrt(experts)
    here_x, here_y = lax.rem(ep, side), lax.div(ep, side)
    local_tokens, width = tokens.shape
    half = width // cores
    chunks = slots // cores
    wide = width // LANES
    thin = half // LANES
    order = far_first(side)
    is_root = ep == 0
    is_late = jnp.logical_and(is_root, c == 0)
    is_mailbox = jnp.logical_and(is_root, c == 1)
    counts_partner = is_root == (c == 0)

    turn = jnp.where(c == 0, 1, side - 1)
    columns_at = [lax.rem(here_x + turn * step, side) for step in range(side)]
    lines_at = [lax.rem(here_y + turn * step, side) * side for step in range(side)]

    def peer(offset):
        return lines_at[offset[1]] + columns_at[offset[0]]

    small = [
        pltpu.make_async_copy(src, dst, small_sem.at[i])
        for i, (src, dst) in enumerate(
            [(route_hbm, route), (tokens_hbm, tokens), (in_gain_hbm, in_gain), (weight_hbm, weight), (out_gain_hbm, out_gain)]
        )
    ]
    for copy in small:
        copy.start()
    barrier = pltpu.get_barrier_semaphore()

    @pl.when(jnp.logical_not(is_late))
    def _():
        for offset in order:
            pl.semaphore_signal(barrier, inc=1, device_id={"ep": peer(offset)}, device_id_type=MESH)

    @pl.when(jnp.logical_not(counts_partner))
    def _():
        pl.semaphore_signal(barrier, inc=1, device_id={"tp": other}, device_id_type=MESH)

    pushes = [
        pltpu.make_async_remote_copy(
            src_ref=src.at[0], dst_ref=dst.at[1], send_sem=push_send.at[i], recv_sem=push_recv.at[i],
            device_id={"tp": other}, device_id_type=MESH,
        )
        for i, (src, dst) in enumerate([(gate_hbm, gate), (up_hbm, up), (down_hbm, down)])
    ]

    def tell_partner():
        pl.semaphore_signal(pair_sem, inc=1, device_id={"tp": other}, device_id_type=MESH)

    def push():
        for copy in pushes:
            copy.start()

    @pl.when(jnp.logical_and(c == 0, is_root))
    def _():
        pl.semaphore_wait(barrier, experts)
        tell_partner()
        push()

    loads = [
        pltpu.make_async_copy(src, dst, weight_sem.at[i])
        for i, (src, dst) in enumerate(
            [
                (sgate_hbm, sgate), (sup_hbm, sup), (sdown_hbm, sdown),
                (gate_hbm.at[0], gate.at[0]), (up_hbm.at[0], up.at[0]), (down_hbm.at[0], down.at[0]),
            ]
        )
    ]
    for copy in loads:
        copy.start()

    small[0].wait()
    names = route[...]
    expert_row = iota((experts, local_tokens), 0)
    hits = [names[k : k + 1, :] == expert_row for k in range(names.shape[0])]
    chosen = functools.reduce(jnp.logical_or, hits)
    earlier = (iota((local_tokens, local_tokens), 0) < iota((local_tokens, local_tokens), 1)).astype(F32).astype(BF16)
    rank_t = jnp.where(chosen, dot(chosen.astype(F32).astype(BF16), earlier), -1.0)

    small[1].wait()
    small[2].wait()
    floats = tokens[...].astype(F32)
    scale = lax.rsqrt(jnp.mean(floats * floats, axis=1, keepdims=True) + EPSILON)
    gains = in_gain[...].astype(F32)
    for q in range(wide):
        lanes = slice(q * LANES, (q + 1) * LANES)
        normed[:, lanes] = (floats[:, lanes] * scale * gains[q : q + 1, :]).astype(BF16)

    to_blocks = one_hot_to_blocks(wide, wide)
    per_block = wide
    first_slot = (c * chunks).astype(F32)
    for j in range(chunks):
        pick = (rank_t == first_slot + j).astype(F32).astype(BF16)
        picked = dot(pick, normed[...]).astype(BF16)
        for b in range(experts // per_block):
            part = picked[b * per_block : (b + 1) * per_block]
            stacked = jnp.concatenate([part[:, q * LANES : (q + 1) * LANES] for q in range(wide)], axis=0)
            tx[j, pl.ds(b * per_block, per_block)] = (
                dot(to_blocks, stacked).astype(BF16).reshape(per_block, wide, LANES)
            )
        rx[j, ep] = tx[j, ep]

    def dispatch(j, to):
        redirect = jnp.logical_and(to == 0, c == 0).astype(jnp.int32)
        return pltpu.make_async_remote_copy(
            src_ref=tx.at[j, to], dst_ref=rx.at[j, ep + redirect * experts], send_sem=send_sem.at[j],
            recv_sem=recv_sem.at[j + redirect * chunks], device_id={"ep": to, "tp": c + redirect}, device_id_type=MESH,
        )

    forwards = [
        pltpu.make_async_remote_copy(
            src_ref=rx.at[j, pl.ds(experts + 1, experts - 1)], dst_ref=rx.at[j, pl.ds(1, experts - 1)],
            send_sem=forward_sem.at[j], recv_sem=recv_sem.at[j], device_id={"tp": 0}, device_id_type=MESH,
        )
        for j in range(chunks)
    ]

    @pl.when(jnp.logical_and(c == 0, jnp.logical_not(is_root)))
    def _():
        pl.semaphore_wait(pair_sem, 1)
        pl.semaphore_wait(barrier, experts - 2)
        tell_partner()

    @pl.when(jnp.logical_and(c == 1, is_root))
    def _():
        pl.semaphore_wait(barrier, experts - 1)

    @pl.when(jnp.logical_and(c == 1, jnp.logical_not(is_root)))
    def _():
        pl.semaphore_wait(barrier, experts)
        tell_partner()

    for j in range(chunks):
        for offset in order:
            dispatch(j, peer(offset)).start()
        if j == 0:

            @pl.when(is_late)
            def _():
                for offset in order:
                    pl.semaphore_signal(late_sem, inc=1, device_id={"ep": peer(offset)}, device_id_type=MESH)

    @pl.when(jnp.logical_and(c == 1, is_root))
    def _():
        pl.semaphore_wait(pair_sem, 1)
        tell_partner()

    @pl.when(jnp.logical_not(is_late))
    def _():
        push()

    def swiglu(inputs, pairs):
        hidden = []
        for gate_here, up_here in pairs:
            gate_value = dot(inputs, gate_here)
            upward = dot(inputs, up_here)
            hidden.append((jax.nn.silu(gate_value) * upward).astype(BF16))
        return hidden

    for copy in loads[:3]:
        copy.wait()
    (hidden,) = swiglu(normed[...], [(sgate[...], sup[...])])
    shared_part = dot(hidden, sdown[...]).astype(BF16)
    for side_of in range(cores):
        shared_send[side_of] = shared_part[:, side_of * half : (side_of + 1) * half]
    pair = pltpu.make_async_remote_copy(
        src_ref=shared_send.at[other], dst_ref=shared_recv, send_sem=pair_send.at[0], recv_sem=pair_recv.at[0],
        device_id={"tp": other}, device_id_type=MESH,
    )
    pair.start()

    small[3].wait()
    small[4].wait()
    weights = weight[...]
    weight_t = functools.reduce(jnp.add, [jnp.where(hit, weights[k : k + 1, :], 0.0) for k, hit in enumerate(hits)])
    high = weight_t.astype(BF16)
    low = (weight_t - high.astype(F32)).astype(BF16)
    eye = (iota((local_tokens, local_tokens), 0) == iota((local_tokens, local_tokens), 1)).astype(F32).astype(BF16)
    turned = [
        lax.dot_general(eye, part, (((1,), (1,)), ((), ())), preferred_element_type=F32).astype(BF16)
        for part in (high, low, rank_t.astype(BF16))
    ]
    columns = experts * cores * thin
    expand = (iota((experts, columns), 0) == iota((experts, columns), 1) // (cores * thin)).astype(F32).astype(BF16)
    spread = dot(jnp.concatenate(turned, axis=0), expand)
    col = iota((local_tokens, columns), 1)
    slot_base = ((col // thin) % cores * chunks).astype(F32)
    q_col = col % thin
    for j in range(chunks):
        here = spread[2 * local_tokens :] == slot_base + j
        for part in range(2):
            value = jnp.where(here, spread[part * local_tokens : (part + 1) * local_tokens], 0.0)
            for q in range(thin):
                picks[j, pl.ds((part * thin + q) * local_tokens, local_tokens)] = jnp.where(
                    q_col == q, value, 0.0
                ).astype(BF16)

    pair.wait()
    for q in range(thin):
        lanes = slice(q * LANES, (q + 1) * LANES)
        total = shared_send[c][:, lanes].astype(F32) + shared_recv[:, lanes].astype(F32)
        shared_half[pl.ds(q * local_tokens, local_tokens)] = total.astype(BF16).astype(F32)

    @pl.when(jnp.logical_and(c == 0, jnp.logical_not(is_root)))
    def _():
        pl.semaphore_wait(late_sem, 1)
        pl.semaphore_signal(late_sem, inc=1, device_id={"tp": 1}, device_id_type=MESH)

    def forward(j):
        @pl.when(is_mailbox)
        def _():
            arrived = rx.at[j, pl.ds(experts + 1, experts - 1)]
            pltpu.make_async_copy(arrived, arrived, recv_sem.at[chunks + j]).wait()
            forwards[j].start()

    forward(0)
    for copy in loads[3:]:
        copy.wait()
    for copy in pushes:
        copy.wait()

    to_rows = one_hot_to_rows(wide, wide)
    per_back = 2 * LANES // thin
    to_thin = one_hot_to_blocks(per_back, thin)

    def give_back(j, offset, core):
        to = peer(offset)
        return pltpu.make_async_remote_copy(
            src_ref=tx2.at[j, core, to], dst_ref=rx2.at[j, ep * cores + c], send_sem=send2_sem.at[j], recv_sem=recv2_sem.at[j],
            device_id={"ep": to, "tp": core}, device_id_type=MESH,
        )

    def to_other_plane(j):
        for offset in order:
            give_back(j, offset, other).start()
        back = pltpu.make_async_remote_copy(
            src_ref=tx2.at[j, other, ep], dst_ref=rx2.at[j, ep * cores + c], send_sem=send2_sem.at[j], recv_sem=recv2_sem.at[j],
            device_id={"tp": other}, device_id_type=MESH,
        )
        back.start()

    for j in range(chunks):
        if j:
            forward(j)
        arrived = rx.at[j, pl.ds(0, experts - 1)]
        pltpu.make_async_copy(arrived, arrived, recv_sem.at[j]).wait()
        for b in range(experts // per_block):
            block = rx[j, pl.ds(b * per_block, per_block)].reshape(per_block * wide, LANES)
            sorted_rows = dot(to_rows, block).astype(BF16)
            for q in range(wide):
                rows[pl.ds(b * per_block, per_block), q * LANES : (q + 1) * LANES] = sorted_rows[
                    q * per_block : (q + 1) * per_block
                ]
        hidden = swiglu(rows[...], [(gate[h], up[h]) for h in range(cores)])
        result = functools.reduce(jnp.add, [dot(hidden[h], down[h]) for h in range(cores)]).astype(BF16)
        for b in range(experts // per_back):
            part = result[b * per_back : (b + 1) * per_back]
            for core in range(cores):
                stacked = jnp.concatenate(
                    [part[:, core * half + q * LANES : core * half + (q + 1) * LANES] for q in range(thin)], axis=0
                )
                tx2[j, core, pl.ds(b * per_back, per_back)] = (
                    dot(to_thin, stacked).astype(BF16).reshape(per_back, thin, LANES)
                )
        for offset in order:
            give_back(j, offset, c).start()
        rx2[j, ep * cores + c] = tx2[j, c, ep]
        if j == 0:

            @pl.when(is_late)
            def _():
                pl.semaphore_wait(pair_sem, 1)

            @pl.when(jnp.logical_and(c == 1, jnp.logical_not(is_root)))
            def _():
                pl.semaphore_wait(pair_sem, 1)
                pl.semaphore_wait(late_sem, 1)

        to_other_plane(j)

    total = shared_half[...]
    for j in range(chunks):
        arrived = rx2.at[j, pl.ds(0, experts * cores - 1)]
        pltpu.make_async_copy(arrived, arrived, recv2_sem.at[j]).wait()
        summed = dot(picks[j], rx2[j].reshape(experts * cores * thin, LANES))
        total = total + summed[: thin * local_tokens] + summed[thin * local_tokens :]
    squares = total * total
    mine = functools.reduce(jnp.add, [squares[q * local_tokens : (q + 1) * local_tokens] for q in range(thin)])
    mine = jnp.broadcast_to(jnp.sum(mine, axis=1, keepdims=True), (local_tokens, LANES))
    sq_send[...] = mine
    pair = pltpu.make_async_remote_copy(
        src_ref=sq_send, dst_ref=sq_recv, send_sem=pair_send.at[1], recv_sem=pair_recv.at[1],
        device_id={"tp": other}, device_id_type=MESH,
    )
    pair.start()
    for j in range(chunks):
        sent = tx.at[j, pl.ds(0, experts - 1)]
        pltpu.make_async_copy(sent, sent, send_sem.at[j]).wait()
        sent = rx2.at[j, pl.ds(0, experts * cores - 1)]
        pltpu.make_async_copy(sent, sent, send2_sem.at[j]).wait()
    @pl.when(is_mailbox)
    def _():
        for copy in forwards:
            copy.wait_send()

    pair.wait()
    scale = lax.rsqrt((mine + sq_recv[...]) / width + EPSILON)
    gains = out_gain[...].astype(F32)
    for q in range(thin):
        lanes = slice(q * LANES, (q + 1) * LANES)
        out_ref[:, lanes] = (total[q * local_tokens : (q + 1) * local_tokens] * scale * gains[q : q + 1, :]).astype(BF16)


def body(tokens, in_gain, route_expert, route_weight, gate_weight, up_weight, down_weight, shared_gate, shared_up, shared_down, out_gain):
    experts, cores = lax.axis_size("ep"), lax.axis_size("tp")
    local_tokens, width = tokens.shape
    top_count = route_expert.shape[1]
    slots = max(2, (local_tokens * top_count * 4 + 3 * experts - 1) // (3 * experts))
    chunks = slots // cores
    half = width // cores
    wide, thin = width // LANES, half // LANES
    hidden = gate_weight.shape[2]
    any_spec = pl.BlockSpec(memory_space=pl.ANY)
    vmem, dma = pltpu.VMEM, pltpu.SemaphoreType.DMA
    scratch = [
        vmem((local_tokens, width), BF16), vmem((wide, LANES), BF16), vmem((top_count, local_tokens), jnp.int32),
        vmem((top_count, local_tokens), F32), vmem((thin, LANES), BF16),
        vmem((cores, width, hidden), BF16), vmem((cores, width, hidden), BF16), vmem((cores, hidden, width), BF16),
        vmem((width, hidden), BF16), vmem((width, hidden), BF16), vmem((hidden, width), BF16),
        vmem((local_tokens, width), BF16),
        vmem((chunks, experts, wide, LANES), BF16), vmem((chunks, 2 * experts, wide, LANES), BF16),
        vmem((experts, width), BF16),
        vmem((chunks, cores, experts, thin, LANES), BF16), vmem((chunks, experts * cores, thin, LANES), BF16),
        vmem((chunks, 2 * thin * local_tokens, experts * cores * thin), BF16),
        vmem((cores, local_tokens, half), BF16), vmem((local_tokens, half), BF16), vmem((thin * local_tokens, LANES), F32),
        vmem((local_tokens, LANES), F32), vmem((local_tokens, LANES), F32),
        dma((5,)), dma((6,)), dma((3,)), dma((3,)), dma((chunks,)), dma((2 * chunks,)), dma((chunks,)), dma((chunks,)),
        dma((chunks,)), dma((2,)), dma((2,)), pltpu.SemaphoreType.REGULAR, pltpu.SemaphoreType.REGULAR,
    ]
    return pl.pallas_call(
        functools.partial(kernel, experts, cores, slots),
        out_shape=jax.ShapeDtypeStruct((local_tokens, half), BF16),
        in_specs=[any_spec] * 11,
        out_specs=pl.BlockSpec(memory_space=pltpu.VMEM),
        scratch_shapes=scratch,
        compiler_params=pltpu.CompilerParams(collective_id=0, has_side_effects=True, vmem_limit_bytes=60 * 1024 * 1024),
    )(
        tokens, in_gain.reshape(wide, LANES), route_expert.T, route_weight.T, gate_weight, up_weight, down_weight,
        shared_gate, shared_up, shared_down, out_gain.reshape(thin, LANES),
    )


def solution(mesh):
    return jax.shard_map(
        body,
        mesh=mesh,
        in_specs=(
            P(("grp", "ep"), None),
            P(),
            P(("grp", "ep"), None),
            P(("grp", "ep"), None),
            P("ep", None, "tp"),
            P("ep", None, "tp"),
            P("ep", "tp", None),
            P(None, "tp"),
            P(None, "tp"),
            P("tp", None),
            P("tp"),
        ),
        out_specs=P(("grp", "ep"), "tp"),
        check_vma=False,
    )
```
